256 devices in a mesh: sp: 16 (over y, x), tp: 16 (over z, core).
Axes of the slice: x: 4, y: 4, z: 8, core: 2. Of those that a mesh axis runs over, the one named last changes fastest.
Arguments:
- queries: bfloat16 [16384, 1536], P('sp', 'tp'), may hold values from -34 to 34
- latent: bfloat16 [16384, 512], P('sp'), may hold values from -6 to 6
- rot_key: bfloat16 [16384, 32], P('sp'), may hold values from -34 to 34
- latent_gain: float32 [512], replicated, may hold values from 0.1 to 1.9
- key_up: bfloat16 [512, 1024], P(None, 'tp'), may hold values from -0.25 to 0.25
- value_up: bfloat16 [512, 1024], P(None, 'tp'), may hold values from -0.70710678 to 0.70710678
- query_gain: float32 [96], replicated, may hold values from 0.5 to 6
- key_gain: float32 [96], replicated, may hold values from 0.5 to 6
- out_gain: float32 [1024], replicated, may hold values from 0.1 to 1.9
- out_weight: bfloat16 [1024, 2048], replicated, may hold values from -0.1875 to 0.1875
- residual: bfloat16 [16384, 2048], P(('sp', 'tp')), may hold values from -6 to 6
- ffn_gain: float32 [2048], replicated, may hold values from 0.1 to 1.9
- routes: int32 [16384, 2], P(('sp', 'tp')), may hold values from 0 to 15, all different within a row; in each aligned block of 64 rows (0 to 63, 64 to 127, ...) at most 9 rows name the same one
- route_weights: float32 [16384, 2], P(('sp', 'tp')), may hold values from 0.2 to 1
- expert_gate: bfloat16 [16, 2048, 2048], P('sp', None, 'tp'), may hold values from -0.125 to 0.125
- expert_up: bfloat16 [16, 2048, 2048], P('sp', None, 'tp'), may hold values from -0.125 to 0.125
- expert_down: bfloat16 [16, 2048, 2048], P('sp', 'tp'), may hold values from -0.125 to 0.125
Outputs:
- layer_out: bfloat16 [16384, 2048], P(('sp', 'tp'))
The draws below stay inside these ranges and needn't reach their ends.
Inputs may be any that keep to these rules, and one draw needn't show every extreme that they name: `routes`: the 2 experts of a token differ. Among the 64 rows of one device each expert is named by at most 9 rows, a bound that some block reaches.
All inputs are finite; a program needn't handle non-finite values.
Results may differ from the reference program's by a relative error of at most 0.02.
The reference program's roundings to bfloat16 on the way count: a program that leaves them out, or rounds other values in their place, can miss the bound.
Values may be sent and summed in bfloat16 or wider, within the bound.
No kernel may reach another device: no remote copies, remote signals or barrier semaphores. Data moves between devices by JAX's collectives and lax.ppermute only.
A program may use at most 128 MiB of HBM per device.

```python
import math
import jax
import jax.numpy as jnp
import numpy as np
from jax import lax

D = 2048
HEADS = 16
NOPE = 64
ROPE = 32
VH = 64
LAT = 512
FF_E = 2048
TOPK = 2
TOK_DEV = 64
QK = 96
ATT_WIDTH = 1024
POS_SP = 1024
LENGTH = 16384
EXPERTS = 16
CAP = 9
N_SP = 16
N_TP = 16


def drawn_pair(key):
    base_query = jnp.clip(jax.random.normal(jax.random.fold_in(key, 11), (LENGTH, HEADS, QK), jnp.float32), -6.0, 6.0)
    base_key = jnp.clip(jax.random.normal(jax.random.fold_in(key, 12), (LENGTH, ROPE), jnp.float32), -6.0, 6.0)
    return (base_query.reshape(LENGTH, HEADS * QK), base_key)


def draw_queries(key, part):
    return drawn_pair(key)[0].astype(jnp.bfloat16)


def draw_rot_key(key, part):
    return drawn_pair(key)[1].astype(jnp.bfloat16)


def head_gains(key):
    spread = 1.0 + 0.18 * jax.random.uniform(jax.random.fold_in(key, 1), (QK,), jnp.float32, -2.5, 2.5)
    return spread


def draw_query_gain(key, part):
    return head_gains(jax.random.fold_in(key, 21))


def draw_key_gain(key, part):
    return head_gains(jax.random.fold_in(key, 22))


def draw_value_up(key, part):
    head_ids = jnp.arange(HEADS * VH, dtype=jnp.int32) // VH
    rising = head_ids.astype(jnp.float32) / max(HEADS - 1, 1)
    entries = jnp.clip(jax.random.normal(jax.random.fold_in(key, 32), (LAT, HEADS * VH), jnp.float32), -4.0, 4.0)
    column_scale = 3.0 ** rising
    return (entries * column_scale[None, :] / jnp.sqrt(jnp.float32(LAT))).astype(jnp.bfloat16)


def shard_levels(rng, extent, shards, smallest, top_value):
    loudness = 1.0
    for position, parts in shards:
        steps = jax.random.uniform(jax.random.fold_in(jax.random.fold_in(rng, 6), position), (parts,), jnp.float32, smallest / len(shards), top_value / len(shards))
        loudness = loudness * jnp.repeat(jnp.exp(steps), extent[position] // parts).reshape((-1,) + (1,) * (len(extent) - 1 - position))
    return loudness


def shared_out(own_key, own, number, rows, number_of, top, reach, lean):
    ranking = jax.random.permutation(own_key, number_of)
    packed, ordinary = load_shares(number_of, rows * top, reach, lean, True), load_shares(number_of, rows * top, reach, lean, False)
    places = jnp.arange(number_of)

    def named(lengths, offset_by):
        used = int((lengths > 0).sum())
        fixed = max(1, used // 4)
        moved = fixed + (places - fixed + offset_by * (used - fixed)) % max(1, number_of - fixed)
        return jnp.zeros((number_of,), jnp.int32).at[ranking[jnp.where(places < fixed, places, moved)]].set(jnp.asarray(lengths, jnp.int32))

    lengths = jnp.where(number % 4 == 0, named(packed, number // 4), named(ordinary, number - number // 4 - 1))
    mixed = jax.random.permutation(jax.random.fold_in(own, 3), number_of)
    giver, sink = mixed[0:number_of // 2 * 2:2], mixed[1:number_of // 2 * 2:2]
    slack = jnp.minimum(lengths[giver] - 1, reach - lengths[sink]) // 2
    slack = jnp.where((giver == ranking[0]) | (sink == ranking[0]) | (lengths[sink] == 0), 0, jnp.maximum(slack, 0))
    moved = jax.random.randint(jax.random.fold_in(own, 4), (number_of // 2,), 0, 1 << 20) % (slack + 1)
    lengths = lengths.at[giver].add(-moved).at[sink].add(moved)
    members = jnp.searchsorted(jnp.cumsum(lengths), jnp.arange(rows * top), side="right").astype(jnp.int32)
    listing = members.reshape(top, rows).T
    listing = listing[jax.random.permutation(jax.random.fold_in(own, 1), rows)]
    offset_by = jax.random.randint(jax.random.fold_in(own, 2), (rows, 1), 0, top)
    return jnp.take_along_axis(listing, (jnp.arange(top)[None, :] + offset_by) % top, axis=1)


def load_shares(number_of, total, bound, slope, full):
    portions = [(1 << 20) // math.isqrt(rank ** slope) + 1 for rank in range(1, number_of + 1)]
    largest = bound if full else min(bound, max(-(-total // number_of), total * portions[0] // sum(portions)))
    least = 1 if total - largest >= number_of - 1 else 0
    given, rest = [largest] + [least] * (number_of - 1), total - largest - least * (number_of - 1)
    while rest > 0:
        candidates = [i for i in range(1, number_of) if given[i] < largest] or [i for i in range(1, number_of) if given[i] < bound]
        pool, budget = sum([portions[i] for i in candidates]), rest
        for i in candidates:
            more = min(bound - given[i], max(1, budget * portions[i] // pool), rest)
            given[i] = given[i] + more
            rest = rest - more
    return np.array(given)


def bell_draw(rng, dims, deviation, bound, split=(), kind=jnp.bfloat16):
    values = deviation * jax.random.normal(rng, dims, jnp.float32)
    if split:
        values = values * shard_levels(rng, dims, split, -0.22, 0.18)
    return jnp.clip(values, -bound, bound).astype(kind)


def setup_inputs(seed: int = 0) -> dict:
    streams_of = jax.random.split(jax.random.key(seed), 18)
    queries = draw_queries(jax.random.fold_in(streams_of[17], 71), 0)
    latent = bell_draw(streams_of[1], (LENGTH, LAT), 1.0, 6.0, ((0, 16),))
    rot_key = draw_rot_key(jax.random.fold_in(streams_of[17], 71), 0)
    latent_gain = jnp.clip(1.0 + 0.18 * jax.random.normal(streams_of[3], (LAT,), jnp.float32), 0.1, 1.9)
    key_up = bell_draw(streams_of[4], (LAT, HEADS * NOPE), LAT ** -0.5, 0.25, ((1, 16),))
    value_up = draw_value_up(jax.random.fold_in(streams_of[17], 71), 0)
    query_gain = draw_query_gain(jax.random.fold_in(streams_of[17], 71), 0)
    key_gain = draw_key_gain(jax.random.fold_in(streams_of[17], 71), 0)
    out_gain = jnp.clip(1.0 + 0.18 * jax.random.normal(streams_of[8], (ATT_WIDTH,), jnp.float32), 0.1, 1.9)
    out_weight = bell_draw(streams_of[9], (ATT_WIDTH, D), ATT_WIDTH ** -0.5, 0.1875)
    residual = bell_draw(streams_of[10], (LENGTH, D), 1.0, 6.0, ((0, 256),))
    ffn_gain = jnp.clip(1.0 + 0.18 * jax.random.normal(streams_of[11], (D,), jnp.float32), 0.1, 1.9)
    routes_keys = jax.random.split(jax.random.fold_in(streams_of[12], 1), LENGTH // TOK_DEV)
    routes_turns = jax.random.permutation(jax.random.fold_in(streams_of[12], 3), LENGTH // TOK_DEV)
    routes = jax.vmap(lambda own, number: shared_out(jax.random.fold_in(streams_of[12], 2), own, number, TOK_DEV, EXPERTS, TOPK, CAP, 1))(routes_keys, routes_turns).reshape((LENGTH, TOPK))
    route_weights = jnp.clip(0.2 + 0.8 * jax.random.uniform(streams_of[13], (LENGTH, TOPK), jnp.float32) ** shard_levels(streams_of[13], (LENGTH, TOPK), ((0, 256),), -0.2, 0.2), 0.2, 1.0)
    expert_gate = bell_draw(streams_of[14], (EXPERTS, D, FF_E), D ** -0.5, 0.125, ((0, 16), (2, 16)))
    expert_up = bell_draw(streams_of[15], (EXPERTS, D, FF_E), D ** -0.5, 0.125, ((0, 16), (2, 16)))
    expert_down = bell_draw(streams_of[16], (EXPERTS, FF_E, D), FF_E ** -0.5, 0.125, ((0, 16), (1, 16)))
    return dict(queries=queries, latent=latent, rot_key=rot_key, latent_gain=latent_gain, key_up=key_up, value_up=value_up, query_gain=query_gain, key_gain=key_gain, out_gain=out_gain, out_weight=out_weight, residual=residual, ffn_gain=ffn_gain, routes=routes, route_weights=route_weights, expert_gate=expert_gate, expert_up=expert_up, expert_down=expert_down)


epsilon = 1e-06
rope_base = 10000.0

def rms_scale(values):
    return lax.rsqrt(lax.optimization_barrier(jnp.mean(values * values, axis=-1, keepdims=True)) + epsilon)

def rotate_half(values, angles):
    half_dims = values.shape[-1] // 2
    first_half = values[..., :half_dims]
    second_half = values[..., half_dims:]
    cosine = jnp.cos(angles)
    sine_val = jnp.sin(angles)
    return jnp.concatenate([first_half * cosine - second_half * sine_val, second_half * cosine + first_half * sine_val], axis=-1)

def head_prepare(raw_rows, gain_vec, angles):
    normed_rows = raw_rows * rms_scale(raw_rows) * gain_vec
    turned_rows = rotate_half(normed_rows[..., NOPE:], angles[:, None, :])
    return jnp.concatenate([normed_rows[..., :NOPE], turned_rows], axis=-1).astype(jnp.bfloat16)

def attend_head(head_inputs):
    query_head, key_head, value_head = head_inputs
    query_f32 = query_head.astype(jnp.float32)
    key_f32 = key_head.astype(jnp.float32)
    value_f32 = value_head.astype(jnp.float32)
    block_count = LENGTH // POS_SP
    query_blocks = query_f32.reshape(block_count, POS_SP, QK)
    key_pos = jnp.arange(LENGTH, dtype=jnp.int32)

    def one_block(block_inputs):
        block_index, query_block = block_inputs
        scores = jnp.dot(query_block, key_f32.T, precision=lax.Precision.HIGHEST) * QK ** (-0.5)
        query_pos = block_index * POS_SP + jnp.arange(POS_SP, dtype=jnp.int32)
        allowed = key_pos[None, :] <= query_pos[:, None]
        scores = jnp.where(allowed, scores, -1e+30)
        row_peak = lax.optimization_barrier(jnp.max(scores, axis=1, keepdims=True))
        exponent = jnp.where(allowed, jnp.exp(scores - row_peak), 0.0)
        row_total = lax.optimization_barrier(jnp.sum(exponent, axis=1))
        rounded_exp = lax.optimization_barrier(exponent.astype(jnp.bfloat16)).astype(jnp.float32)
        result = jnp.dot(rounded_exp, value_f32, precision=lax.Precision.HIGHEST) / row_total[:, None]
        return result.astype(jnp.bfloat16)
    outputs = lax.map(one_block, (jnp.arange(block_count, dtype=jnp.int32), query_blocks))
    return outputs.reshape(LENGTH, VH)

def reference(queries, latent, rot_key, latent_gain, key_up, value_up, query_gain, key_gain, out_gain, out_weight, residual, ffn_gain, routes, route_weights, expert_gate, expert_up, expert_down):
    lat_f32 = latent.astype(jnp.float32)
    normed_latent = (lat_f32 * rms_scale(lat_f32) * latent_gain).astype(jnp.bfloat16)
    key_nope = jnp.dot(normed_latent, key_up, preferred_element_type=jnp.float32).astype(jnp.bfloat16)
    values = jnp.dot(normed_latent, value_up, preferred_element_type=jnp.float32).astype(jnp.bfloat16)
    positions = jnp.arange(LENGTH, dtype=jnp.int32)
    inverse = rope_base ** (-jnp.arange(0, ROPE, 2, dtype=jnp.float32) / ROPE)
    angles = positions.astype(jnp.float32)[:, None] * inverse[None, :]
    shared = jnp.broadcast_to(rot_key.astype(jnp.float32)[:, None, :], (LENGTH, HEADS, ROPE))
    raw_keys = jnp.concatenate([key_nope.astype(jnp.float32).reshape(LENGTH, HEADS, NOPE), shared], axis=-1)
    key_rows = head_prepare(raw_keys, key_gain, angles)
    query_rows = head_prepare(queries.astype(jnp.float32).reshape(LENGTH, HEADS, QK), query_gain, angles)
    value_heads = values.reshape(LENGTH, HEADS, VH)
    attended = lax.map(attend_head, (jnp.transpose(query_rows, (1, 0, 2)), jnp.transpose(key_rows, (1, 0, 2)), jnp.transpose(value_heads, (1, 0, 2))))
    att_rows = jnp.transpose(attended, (1, 0, 2)).reshape(LENGTH, ATT_WIDTH).astype(jnp.float32)
    normed_att = (att_rows * rms_scale(att_rows) * out_gain).astype(jnp.bfloat16)
    group_width = ATT_WIDTH // N_TP
    mixed = jnp.zeros((LENGTH, D), jnp.float32)
    for group_index in range(N_TP):
        low = group_index * group_width
        partial_value = jnp.dot(normed_att[:, low:low + group_width], out_weight[low:low + group_width], preferred_element_type=jnp.float32).astype(jnp.bfloat16)
        mixed = mixed + lax.optimization_barrier(partial_value).astype(jnp.float32)
    middle = residual.astype(jnp.float32) + mixed
    ffn_input = (middle * rms_scale(middle) * ffn_gain).astype(jnp.bfloat16)
    flat_routes = routes.reshape(-1).astype(jnp.int32)
    row_order = jnp.argsort(flat_routes, stable=True).astype(jnp.int32)
    expert_counts = lax.optimization_barrier(jnp.sum((flat_routes[:, None] == jnp.arange(EXPERTS, dtype=jnp.int32)[None, :]).astype(jnp.int32), axis=0))
    offsets = (jnp.cumsum(expert_counts) - expert_counts).astype(jnp.int32)
    row_limit = N_SP * N_TP * CAP
    weights_flat = route_weights.reshape(-1).astype(jnp.float32)
    hidden_width = FF_E // N_TP

    def per_expert(expert_id, combined):
        slot_ids = jnp.arange(row_limit, dtype=jnp.int32)
        is_live = slot_ids < expert_counts[expert_id]
        picked = row_order[jnp.minimum(offsets[expert_id] + slot_ids, LENGTH * TOPK - 1)]
        token_ids = (picked // TOPK).astype(jnp.int32)
        expert_in = ffn_input[token_ids]
        gate_pre = jnp.dot(expert_in, expert_gate[expert_id], preferred_element_type=jnp.float32)
        up_pre = jnp.dot(expert_in, expert_up[expert_id], preferred_element_type=jnp.float32)
        hidden = (jax.nn.silu(gate_pre) * up_pre).astype(jnp.bfloat16)
        down_weight = expert_down[expert_id]
        down_sum = jnp.zeros((row_limit, D), jnp.float32)
        for group_index in range(N_TP):
            low = group_index * hidden_width
            partial_value = jnp.dot(hidden[:, low:low + hidden_width], down_weight[low:low + hidden_width], preferred_element_type=jnp.float32).astype(jnp.bfloat16)
            down_sum = down_sum + lax.optimization_barrier(partial_value).astype(jnp.float32)
        expert_out = lax.optimization_barrier(down_sum.astype(jnp.bfloat16)).astype(jnp.float32)
        contrib_rows = expert_out * (weights_flat[picked] * is_live.astype(jnp.float32))[:, None]
        return combined.at[token_ids].add(contrib_rows)
    combined = lax.fori_loop(0, EXPERTS, per_expert, jnp.zeros((LENGTH, D), jnp.float32))
    return (middle + combined).astype(jnp.bfloat16)
```

```python
import jax
import jax.numpy as jnp
from jax import lax
from jax.experimental import pallas as pl
from jax.experimental.pallas import tpu as pltpu
from jax.sharding import PartitionSpec as P

D = 2048
NOPE = 64
ROPE = 32
VH = 64
TOPK = 2
QK = 96
SIDE = 4
LOG2E = 1.4426950408889634
LOW = -1e30


epsilon = 1e-06
rope_base = 10000.0


def rms_scale(values):
    return lax.rsqrt(jnp.mean(values * values, axis=-1, keepdims=True) + epsilon)


def head_prepare(raw, gain_vec, cosine, sine_val):
    scale = lax.rsqrt(jnp.mean(raw * raw, axis=0, keepdims=True) + epsilon)
    normed = raw * scale * gain_vec[:, None]
    first = normed[NOPE : NOPE + ROPE // 2]
    second = normed[NOPE + ROPE // 2 :]
    return jnp.concatenate(
        [normed[:NOPE], first * cosine - second * sine_val, second * cosine + first * sine_val],
        axis=0,
    ).astype(jnp.bfloat16)


def attend_kernel(qs_ref, ks_ref, *refs, tq, tk, parts):
    q_in, kv_in = refs[:parts], refs[parts : 2 * parts]
    out_ref = refs[2 * parts]
    q_buf, kv_buf, k_nat, v_aug, acc, peak, sems = refs[2 * parts + 1 :]
    span = kv_buf.shape[2]
    copies = []
    for i in range(parts):
        for j, (src, dst) in enumerate(((kv_in[i], kv_buf.at[i]), (q_in[i], q_buf.at[i]))):
            copy = pltpu.make_async_copy(src, dst, sems.at[2 * i + j])
            copy.start()
            copies.append(copy)
    for i in range(parts):
        copies[2 * i].wait()
        k_nat[pl.ds(i * span, span), :] = kv_buf[i, :QK, :].astype(jnp.float32).T.astype(jnp.bfloat16)
        for j in range(span // tk):
            piece = i * (span // tk) + j
            v_aug[piece, :VH, :] = kv_buf[i, QK:, j * tk : (j + 1) * tk]
            v_aug[piece, VH:, :] = jnp.ones((16, tk), jnp.bfloat16)
    for i in range(parts):
        copies[2 * i + 1].wait()

    scale = LOG2E * QK ** (-0.5)
    per_q = span // tq
    per_k = span // tk

    def q_tile(t, carry):
        i, h = t // per_q, t % per_q
        q_start = qs_ref[t]
        q = q_buf[i, :, pl.ds(pl.multiple_of(h * tq, tq), tq)]
        acc[...] = jnp.zeros_like(acc)
        peak[...] = jnp.full_like(peak, LOW)

        def k_tile(u, c):
            k_start = ks_ref[u // per_k] + (u % per_k) * tk

            def update(masked):
                keys = k_nat[pl.ds(pl.multiple_of(u * tk, tk), tk), :]
                s = jnp.dot(keys, q, preferred_element_type=jnp.float32) * scale
                if masked:
                    kpos = k_start + lax.broadcasted_iota(jnp.int32, s.shape, 0)
                    qpos = q_start + lax.broadcasted_iota(jnp.int32, s.shape, 1)
                    s = jnp.where(kpos <= qpos, s, LOW)
                old = peak[0:1, :]
                new = jnp.maximum(old, jnp.max(s, axis=0, keepdims=True))
                e = jnp.exp2(s - new).astype(jnp.bfloat16)
                part = jnp.dot(v_aug[u], e, preferred_element_type=jnp.float32)
                acc[...] = acc[...] * jnp.exp2(old - new) + part
                peak[...] = jnp.broadcast_to(new, peak.shape)

            @pl.when(k_start + tk - 1 <= q_start)
            def _():
                update(False)

            @pl.when((k_start + tk - 1 > q_start) & (k_start <= q_start + tq - 1))
            def _():
                update(True)

            return c

        lax.fori_loop(0, parts * per_k, k_tile, 0)
        total = acc[VH : VH + 1, :]
        live = total > 0.0
        safe = jnp.where(live, total, 1.0)
        lse = jnp.where(live, peak[0:1, :] + jnp.log2(safe), LOW)
        hi = lse.astype(jnp.bfloat16)
        mid = (lse - hi.astype(jnp.float32)).astype(jnp.bfloat16)
        lo = (lse - hi.astype(jnp.float32) - mid.astype(jnp.float32)).astype(jnp.bfloat16)
        row = lax.broadcasted_iota(jnp.int32, (16, tq), 0)
        stats = jnp.where(
            row == 0,
            hi.astype(jnp.float32),
            jnp.where(row == 1, mid.astype(jnp.float32), jnp.where(row == 2, lo.astype(jnp.float32), 0.0)),
        )
        cols = pl.ds(pl.multiple_of(h * tq, tq), tq)
        out_ref[i, :VH, cols] = (acc[:VH, :] / safe).astype(jnp.bfloat16)
        out_ref[i, VH:, cols] = stats.astype(jnp.bfloat16)
        return carry

    lax.fori_loop(0, parts * per_q, q_tile, 0)


def attend(q_parts, kv_parts, q_starts, k_starts, tq=512, tk=512):
    parts = len(q_parts)
    span = q_parts[0].shape[1]
    hbm = pl.BlockSpec(memory_space=pl.ANY)
    smem = pl.BlockSpec(memory_space=pltpu.SMEM)

    def kernel(*refs):
        attend_kernel(*refs, tq=tq, tk=tk, parts=parts)

    work = parts * parts * span * span // 2
    return pl.pallas_call(
        kernel,
        out_shape=jax.ShapeDtypeStruct((parts, VH + 16, span), jnp.bfloat16),
        in_specs=[smem, smem] + [hbm] * (2 * parts),
        out_specs=pl.BlockSpec(memory_space=pltpu.VMEM),
        scratch_shapes=[
            pltpu.VMEM((parts, QK, span), jnp.bfloat16),
            pltpu.VMEM((parts, QK + VH, span), jnp.bfloat16),
            pltpu.VMEM((parts * span, QK), jnp.bfloat16),
            pltpu.VMEM((parts * span // tk, VH + 16, tk), jnp.bfloat16),
            pltpu.VMEM((VH + 16, tq), jnp.float32),
            pltpu.VMEM((8, tq), jnp.float32),
            pltpu.SemaphoreType.DMA((2 * parts,)),
        ],
        compiler_params=pltpu.CompilerParams(vmem_limit_bytes=48 * 1024 * 1024),
        cost_estimate=pl.CostEstimate(
            flops=2 * work * (QK + VH), bytes_accessed=3 * 1024 * 1024, transcendentals=work
        ),
        name="attend",
    )(q_starts, k_starts, *q_parts, *kv_parts)


def expert_kernel(x_ref, g_ref, u_ref, d_ref, o_ref, acc):
    step = pl.program_id(0)
    pairs = g_ref.shape[0]
    weights = jnp.concatenate(
        [g_ref[i] for i in range(pairs)] + [u_ref[i] for i in range(pairs)], axis=1
    )
    both = jnp.dot(x_ref[...], weights, preferred_element_type=jnp.float32)
    half = both.shape[1] // 2
    gate, up = both[:, :half], both[:, half:]
    hidden = (gate / (1.0 + jnp.exp(-gate)) * up).astype(jnp.bfloat16)
    part = jnp.dot(hidden, d_ref[...], preferred_element_type=jnp.float32)

    @pl.when(step == 0)
    def _():
        acc[...] = part

    @pl.when(step > 0)
    def _():
        acc[...] += part

    @pl.when(step == pl.num_programs(0) - 1)
    def _():
        o_ref[...] = acc[...].astype(jnp.bfloat16)


def expert_ffn(rows, gate, up, down):
    slices, _, width = gate.shape
    pairs = 2
    count = rows.shape[0]
    return pl.pallas_call(
        expert_kernel,
        out_shape=jax.ShapeDtypeStruct((count, D), jnp.bfloat16),
        grid=(slices // pairs,),
        in_specs=[
            pl.BlockSpec((count, D), lambda i: (0, 0)),
            pl.BlockSpec((pairs, D, width), lambda i: (i, 0, 0)),
            pl.BlockSpec((pairs, D, width), lambda i: (i, 0, 0)),
            pl.BlockSpec((pairs * width, D), lambda i: (i, 0)),
        ],
        out_specs=pl.BlockSpec((count, D), lambda i: (0, 0)),
        scratch_shapes=[pltpu.VMEM((count, D), jnp.float32)],
        compiler_params=pltpu.CompilerParams(
            dimension_semantics=("arbitrary",), vmem_limit_bytes=40 * 1024 * 1024
        ),
        cost_estimate=pl.CostEstimate(
            flops=6 * count * D * slices * width,
            bytes_accessed=6 * D * slices * width,
            transcendentals=count * slices * width,
        ),
        name="expert_ffn",
    )(rows, gate, up, down)


def slot_targets(route_rows, expert_total, slot_cap):
    flat_routes = route_rows.reshape(-1)
    one_hot = (flat_routes[:, None] == jnp.arange(expert_total, dtype=jnp.int32)[None, :]).astype(
        jnp.int32
    )
    earlier = jnp.cumsum(one_hot, axis=0) - one_hot
    rank_in = jnp.sum(earlier * one_hot, axis=1)
    return (flat_routes * slot_cap + rank_in).reshape(route_rows.shape)


def select_matrix(targets, slot_total):
    hits = targets[:, :, None] == jnp.arange(slot_total, dtype=jnp.int32)[None, None, :]
    return jnp.sum(hits.astype(jnp.bfloat16), axis=1)


def row_shift(value, k):
    pairs = [
        (y * SIDE + x, y * SIDE + (x + k) % SIDE) for y in range(SIDE) for x in range(SIDE)
    ]
    return lax.ppermute(value, "sp", pairs)


def column_shift(value, k):
    pairs = [
        (y * SIDE + x, ((y + k) % SIDE) * SIDE + x) for y in range(SIDE) for x in range(SIDE)
    ]
    return lax.ppermute(value, "sp", pairs)


def row_swap(value):
    pairs = [
        (y * SIDE + x, (SIDE - 1 - y) * SIDE + x) for y in range(SIDE) for x in range(SIDE)
    ]
    return lax.ppermute(value, "sp", pairs)


def shards(
    queries,
    latent,
    rot_key,
    latent_gain,
    key_up,
    value_up,
    query_gain,
    key_gain,
    out_gain,
    out_weight,
    residual,
    ffn_gain,
    routes,
    route_weights,
    expert_gate,
    expert_up,
    expert_down,
):
    shard_len = queries.shape[0]
    half_len = shard_len // 2
    sp_count = lax.axis_size("sp")
    me = lax.axis_index("sp")
    my_y, my_x = me // SIDE, me % SIDE

    gate_all = lax.all_gather(expert_gate[0], "tp", axis=0, tiled=False)
    up_all = lax.all_gather(expert_up[0], "tp", axis=0, tiled=False)
    down_all = lax.all_gather(expert_down[0], "tp", axis=0, tiled=True)

    positions = me * shard_len + jnp.arange(shard_len, dtype=jnp.int32)
    inverse = rope_base ** (-jnp.arange(0, ROPE, 2, dtype=jnp.float32) / ROPE)
    angles = positions.astype(jnp.float32)[None, :] * inverse[:, None]
    cosine, sine_val = jnp.cos(angles), jnp.sin(angles)

    query_rows = head_prepare(queries.astype(jnp.float32).T, query_gain, cosine, sine_val)
    swapped = row_swap(query_rows[:, half_len:])
    q_set = jnp.concatenate([query_rows[:, :half_len], swapped], axis=1)

    lat_f32 = latent.astype(jnp.float32)
    normed_latent = (lat_f32 * rms_scale(lat_f32) * latent_gain).astype(jnp.bfloat16)
    both_up = jnp.concatenate([key_up, value_up], axis=1)
    lifted = lax.dot_general(
        both_up, normed_latent, (((0,), (1,)), ((), ())), preferred_element_type=jnp.float32
    ).astype(jnp.bfloat16)
    raw_keys = jnp.concatenate(
        [lifted[:NOPE].astype(jnp.float32), rot_key.astype(jnp.float32).T], axis=0
    )
    bundle = jnp.concatenate(
        [head_prepare(raw_keys, key_gain, cosine, sine_val), lifted[NOPE:]], axis=0
    )

    shifts = range(SIDE)
    kv_parts = [bundle] + [column_shift(bundle, k) for k in shifts[1:]]
    q_parts = [q_set] + [row_shift(q_set, k) for k in shifts[1:]]
    k_starts = jnp.stack([((my_y - k) % SIDE * SIDE + my_x) * shard_len for k in shifts])
    q_cols = [(my_x - k) % SIDE for k in shifts]
    q_starts = jnp.stack(
        sum(
            [
                [
                    (my_y * SIDE + c) * shard_len,
                    ((SIDE - 1 - my_y) * SIDE + c) * shard_len + half_len,
                ]
                for c in q_cols
            ],
            [],
        )
    )
    partial = attend(q_parts, kv_parts, q_starts.astype(jnp.int32), k_starts.astype(jnp.int32))
    pieces = [partial[0]] + [row_shift(partial[k], -k) for k in shifts[1:]]
    levels = [jnp.sum(p[VH : VH + 3].astype(jnp.float32), axis=0, keepdims=True) for p in pieces]
    top = levels[0]
    for level in levels[1:]:
        top = jnp.maximum(top, level)
    shares = [jnp.exp2(level - top) for level in levels]
    merged = sum(w * p[:VH].astype(jnp.float32) for w, p in zip(shares, pieces)) / sum(shares)
    merged = merged.astype(jnp.bfloat16)
    back = row_swap(merged[:, half_len:])
    attended = jnp.concatenate([merged[:, :half_len], back], axis=1)

    tok_count = residual.shape[0]
    token_rows = lax.all_to_all(
        attended.T, "tp", split_axis=0, concat_axis=1, tiled=True
    ).astype(jnp.float32)
    normed_rows = (token_rows * rms_scale(token_rows) * out_gain).astype(jnp.bfloat16)
    mixed = jnp.dot(normed_rows, out_weight, preferred_element_type=jnp.float32)
    middle = residual.astype(jnp.float32) + mixed
    ffn_input = (middle * rms_scale(middle) * ffn_gain).astype(jnp.bfloat16)
    slot_cap = max(2, 9 * tok_count * TOPK // (8 * sp_count))
    slot_total = sp_count * slot_cap
    targets = slot_targets(routes, sp_count, slot_cap)
    chooser = select_matrix(targets, slot_total)
    outbound = (
        jnp.einsum("ts,td->sd", chooser, ffn_input, preferred_element_type=jnp.float32)
        .astype(jnp.bfloat16)
        .reshape(sp_count, slot_cap, D)
    )
    arrived = lax.all_to_all(outbound, "sp", split_axis=0, concat_axis=0, tiled=True)
    served = expert_ffn(arrived.reshape(slot_total, D), gate_all, up_all, down_all)
    returned_rows = lax.all_to_all(
        served.reshape(sp_count, slot_cap, D), "sp", split_axis=0, concat_axis=0, tiled=True
    ).reshape(slot_total, D)
    picked = (
        jnp.take(returned_rows, targets.reshape(-1), axis=0)
        .reshape(tok_count, TOPK, D)
        .astype(jnp.float32)
    )
    moe_sum = jnp.sum(picked * route_weights[:, :, None], axis=1)
    return (middle + moe_sum).astype(jnp.bfloat16)


def solution(mesh):
    return jax.shard_map(
        shards,
        mesh=mesh,
        in_specs=(
            P("sp", "tp"),
            P("sp", None),
            P("sp", None),
            P(),
            P(None, "tp"),
            P(None, "tp"),
            P(),
            P(),
            P(),
            P(),
            P(("sp", "tp"), None),
            P(),
            P(("sp", "tp"), None),
            P(("sp", "tp"), None),
            P("sp", None, "tp"),
            P("sp", None, "tp"),
            P("sp", "tp", None),
        ),
        out_specs=P(("sp", "tp"), None),
        check_vma=False,
    )
```

```python
import jax
import jax.numpy as jnp
from jax import lax
from jax.experimental import pallas as pl
from jax.experimental.pallas import tpu as pltpu
from jax.sharding import PartitionSpec as P

D = 2048
NOPE = 64
ROPE = 32
VH = 64
TOPK = 2
QK = 96
CORES = 2
SIDE = 4
LOG2E = 1.4426950408889634
LOW = -1e30


epsilon = 1e-06
rope_base = 10000.0


def rms_scale(values):
    return lax.rsqrt(jnp.mean(values * values, axis=-1, keepdims=True) + epsilon)


def head_prepare(raw, gain_vec, cosine, sine_val):
    scale = lax.rsqrt(jnp.mean(raw * raw, axis=0, keepdims=True) + epsilon)
    normed = raw * scale * gain_vec[:, None]
    first = normed[NOPE : NOPE + ROPE // 2]
    second = normed[NOPE + ROPE // 2 :]
    return jnp.concatenate(
        [normed[:NOPE], first * cosine - second * sine_val, second * cosine + first * sine_val],
        axis=0,
    ).astype(jnp.bfloat16)


def attend_kernel(qs_ref, ks_ref, *refs, tq, tk, parts):
    q_in, kv_in = refs[:parts], refs[parts : 2 * parts]
    out_ref = refs[2 * parts]
    q_buf, kv_buf, k_nat, v_aug, acc, peak, sems = refs[2 * parts + 1 :]
    span = kv_buf.shape[2]
    copies = []
    for i in range(parts):
        for j, (src, dst) in enumerate(((kv_in[i], kv_buf.at[i]), (q_in[i], q_buf.at[i]))):
            copy = pltpu.make_async_copy(src, dst, sems.at[2 * i + j])
            copy.start()
            copies.append(copy)
    for i in range(parts):
        copies[2 * i].wait()
        k_nat[pl.ds(i * span, span), :] = kv_buf[i, :QK, :].astype(jnp.float32).T.astype(jnp.bfloat16)
        for j in range(span // tk):
            piece = i * (span // tk) + j
            v_aug[piece, :VH, :] = kv_buf[i, QK:, j * tk : (j + 1) * tk]
            v_aug[piece, VH:, :] = jnp.ones((16, tk), jnp.bfloat16)
    for i in range(parts):
        copies[2 * i + 1].wait()

    scale = LOG2E * QK ** (-0.5)
    per_q = span // tq
    per_k = span // tk

    def q_tile(t, carry):
        i, h = t // per_q, t % per_q
        q_start = qs_ref[t]
        q = q_buf[i, :, pl.ds(pl.multiple_of(h * tq, tq), tq)]
        acc[...] = jnp.zeros_like(acc)
        peak[...] = jnp.full_like(peak, LOW)

        def k_tile(u, c):
            k_start = ks_ref[u // per_k] + (u % per_k) * tk

            def update(masked):
                keys = k_nat[pl.ds(pl.multiple_of(u * tk, tk), tk), :]
                s = jnp.dot(keys, q, preferred_element_type=jnp.float32) * scale
                if masked:
                    kpos = k_start + lax.broadcasted_iota(jnp.int32, s.shape, 0)
                    qpos = q_start + lax.broadcasted_iota(jnp.int32, s.shape, 1)
                    s = jnp.where(kpos <= qpos, s, LOW)
                old = peak[0:1, :]
                new = jnp.maximum(old, jnp.max(s, axis=0, keepdims=True))
                e = jnp.exp2(s - new).astype(jnp.bfloat16)
                part = jnp.dot(v_aug[u], e, preferred_element_type=jnp.float32)
                acc[...] = acc[...] * jnp.exp2(old - new) + part
                peak[...] = jnp.broadcast_to(new, peak.shape)

            @pl.when(k_start + tk - 1 <= q_start)
            def _():
                update(False)

            @pl.when((k_start + tk - 1 > q_start) & (k_start <= q_start + tq - 1))
            def _():
                update(True)

            return c

        lax.fori_loop(0, parts * per_k, k_tile, 0)
        total = acc[VH : VH + 1, :]
        live = total > 0.0
        safe = jnp.where(live, total, 1.0)
        lse = jnp.where(live, peak[0:1, :] + jnp.log2(safe), LOW)
        hi = lse.astype(jnp.bfloat16)
        mid = (lse - hi.astype(jnp.float32)).astype(jnp.bfloat16)
        lo = (lse - hi.astype(jnp.float32) - mid.astype(jnp.float32)).astype(jnp.bfloat16)
        row = lax.broadcasted_iota(jnp.int32, (16, tq), 0)
        stats = jnp.where(
            row == 0,
            hi.astype(jnp.float32),
            jnp.where(row == 1, mid.astype(jnp.float32), jnp.where(row == 2, lo.astype(jnp.float32), 0.0)),
        )
        cols = pl.ds(pl.multiple_of(h * tq, tq), tq)
        out_ref[i, :VH, cols] = (acc[:VH, :] / safe).astype(jnp.bfloat16)
        out_ref[i, VH:, cols] = stats.astype(jnp.bfloat16)
        return carry

    lax.fori_loop(0, parts * per_q, q_tile, 0)


def attend(q_parts, kv_parts, q_starts, k_starts, tq=512, tk=512):
    parts = len(q_parts)
    span = q_parts[0].shape[1]
    hbm = pl.BlockSpec(memory_space=pl.ANY)
    smem = pl.BlockSpec(memory_space=pltpu.SMEM)

    def kernel(*refs):
        attend_kernel(*refs, tq=tq, tk=tk, parts=parts)

    work = parts * parts * span * span // 2
    return pl.pallas_call(
        kernel,
        out_shape=jax.ShapeDtypeStruct((parts, VH + 16, span), jnp.bfloat16),
        in_specs=[smem, smem] + [hbm] * (2 * parts),
        out_specs=pl.BlockSpec(memory_space=pltpu.VMEM),
        scratch_shapes=[
            pltpu.VMEM((parts, QK, span), jnp.bfloat16),
            pltpu.VMEM((parts, QK + VH, span), jnp.bfloat16),
            pltpu.VMEM((parts * span, QK), jnp.bfloat16),
            pltpu.VMEM((parts * span // tk, VH + 16, tk), jnp.bfloat16),
            pltpu.VMEM((VH + 16, tq), jnp.float32),
            pltpu.VMEM((8, tq), jnp.float32),
            pltpu.SemaphoreType.DMA((2 * parts,)),
        ],
        compiler_params=pltpu.CompilerParams(vmem_limit_bytes=48 * 1024 * 1024),
        cost_estimate=pl.CostEstimate(
            flops=2 * work * (QK + VH), bytes_accessed=3 * 1024 * 1024, transcendentals=work
        ),
        name="attend",
    )(q_starts, k_starts, *q_parts, *kv_parts)


def lift_kernel(x_ref, g_ref, u_ref, o_ref):
    pairs = g_ref.shape[0]
    weights = jnp.concatenate(
        [g_ref[i] for i in range(pairs)] + [u_ref[i] for i in range(pairs)], axis=1
    )
    both = jnp.dot(x_ref[...], weights, preferred_element_type=jnp.float32)
    half = both.shape[1] // 2
    gate, up = both[:, :half], both[:, half:]
    o_ref[...] = (gate / (1.0 + jnp.exp(-gate)) * up).astype(jnp.bfloat16)


def expert_lift(rows, gate, up):
    slices, _, width = gate.shape
    pairs = 2
    count = rows.shape[0]
    return pl.pallas_call(
        lift_kernel,
        out_shape=jax.ShapeDtypeStruct((count, slices * width), jnp.bfloat16),
        grid=(slices // pairs,),
        in_specs=[
            pl.BlockSpec((count, D), lambda i: (0, 0)),
            pl.BlockSpec((pairs, D, width), lambda i: (i, 0, 0)),
            pl.BlockSpec((pairs, D, width), lambda i: (i, 0, 0)),
        ],
        out_specs=pl.BlockSpec((count, pairs * width), lambda i: (0, i)),
        compiler_params=pltpu.CompilerParams(
            dimension_semantics=("arbitrary",), vmem_limit_bytes=32 * 1024 * 1024
        ),
        cost_estimate=pl.CostEstimate(
            flops=4 * count * D * slices * width,
            bytes_accessed=4 * D * slices * width,
            transcendentals=count * slices * width,
        ),
        name="expert_lift",
    )(rows, gate, up)


def lower_kernel(h_ref, d_ref, o_ref):
    o_ref[...] = jnp.dot(h_ref[...], d_ref[...], preferred_element_type=jnp.float32).astype(
        jnp.bfloat16
    )


def expert_lower(hidden, down):
    count, width = hidden.shape
    cols = 512
    return pl.pallas_call(
        lower_kernel,
        out_shape=jax.ShapeDtypeStruct((count, D), jnp.bfloat16),
        grid=(D // cols,),
        in_specs=[
            pl.BlockSpec((count, width), lambda i: (0, 0)),
            pl.BlockSpec((width, cols), lambda i: (0, i)),
        ],
        out_specs=pl.BlockSpec((count, cols), lambda i: (0, i)),
        compiler_params=pltpu.CompilerParams(
            dimension_semantics=("arbitrary",), vmem_limit_bytes=32 * 1024 * 1024
        ),
        cost_estimate=pl.CostEstimate(
            flops=2 * count * D * width, bytes_accessed=2 * D * width, transcendentals=0
        ),
        name="expert_lower",
    )(hidden, down)


def slot_targets(route_rows, expert_total, slot_cap):
    flat_routes = route_rows.reshape(-1)
    one_hot = (flat_routes[:, None] == jnp.arange(expert_total, dtype=jnp.int32)[None, :]).astype(
        jnp.int32
    )
    earlier = jnp.cumsum(one_hot, axis=0) - one_hot
    rank_in = jnp.sum(earlier * one_hot, axis=1)
    return (flat_routes * slot_cap + rank_in).reshape(route_rows.shape)


def select_matrix(targets, slot_total):
    hits = targets[:, :, None] == jnp.arange(slot_total, dtype=jnp.int32)[None, None, :]
    return jnp.sum(hits.astype(jnp.bfloat16), axis=1)


def row_shift(value, k):
    pairs = [
        (y * SIDE + x, y * SIDE + (x + k) % SIDE) for y in range(SIDE) for x in range(SIDE)
    ]
    return lax.ppermute(value, "sp", pairs)


def column_shift(value, k):
    pairs = [
        (y * SIDE + x, ((y + k) % SIDE) * SIDE + x) for y in range(SIDE) for x in range(SIDE)
    ]
    return lax.ppermute(value, "sp", pairs)


def row_swap(value):
    pairs = [
        (y * SIDE + x, (SIDE - 1 - y) * SIDE + x) for y in range(SIDE) for x in range(SIDE)
    ]
    return lax.ppermute(value, "sp", pairs)


def core_swap(value):
    pairs = [(t, t ^ 1) for t in range(lax.axis_size("tp"))]
    return lax.ppermute(value, "tp", pairs)


def shards(
    queries,
    latent,
    rot_key,
    latent_gain,
    key_up,
    value_up,
    query_gain,
    key_gain,
    out_gain,
    out_weight,
    residual,
    ffn_gain,
    routes,
    route_weights,
    expert_gate,
    expert_up,
    expert_down,
):
    shard_len = queries.shape[0]
    half_len = shard_len // 2
    sp_count = lax.axis_size("sp")
    me = lax.axis_index("sp")
    my_y, my_x = me // SIDE, me % SIDE

    same_core = [list(range(c, lax.axis_size("tp"), CORES)) for c in range(CORES)]

    def collect(weights):
        return lax.all_gather(weights, "tp", axis_index_groups=same_core, axis=0, tiled=False)

    gate_all = collect(expert_gate[0])
    up_all = collect(expert_up[0])
    down_all = collect(expert_down[0])

    positions = me * shard_len + jnp.arange(shard_len, dtype=jnp.int32)
    inverse = rope_base ** (-jnp.arange(0, ROPE, 2, dtype=jnp.float32) / ROPE)
    angles = positions.astype(jnp.float32)[None, :] * inverse[:, None]
    cosine, sine_val = jnp.cos(angles), jnp.sin(angles)

    query_rows = head_prepare(queries.astype(jnp.float32).T, query_gain, cosine, sine_val)
    swapped = row_swap(query_rows[:, half_len:])
    q_set = jnp.concatenate([query_rows[:, :half_len], swapped], axis=1)

    lat_f32 = latent.astype(jnp.float32)
    normed_latent = (lat_f32 * rms_scale(lat_f32) * latent_gain).astype(jnp.bfloat16)
    both_up = jnp.concatenate([key_up, value_up], axis=1)
    lifted = lax.dot_general(
        both_up, normed_latent, (((0,), (1,)), ((), ())), preferred_element_type=jnp.float32
    ).astype(jnp.bfloat16)
    raw_keys = jnp.concatenate(
        [lifted[:NOPE].astype(jnp.float32), rot_key.astype(jnp.float32).T], axis=0
    )
    bundle = jnp.concatenate(
        [head_prepare(raw_keys, key_gain, cosine, sine_val), lifted[NOPE:]], axis=0
    )

    shifts = range(SIDE)
    kv_parts = [bundle] + [column_shift(bundle, k) for k in shifts[1:]]
    q_parts = [q_set] + [row_shift(q_set, k) for k in shifts[1:]]
    k_starts = jnp.stack([((my_y - k) % SIDE * SIDE + my_x) * shard_len for k in shifts])
    q_cols = [(my_x - k) % SIDE for k in shifts]
    q_starts = jnp.stack(
        sum(
            [
                [
                    (my_y * SIDE + c) * shard_len,
                    ((SIDE - 1 - my_y) * SIDE + c) * shard_len + half_len,
                ]
                for c in q_cols
            ],
            [],
        )
    )
    partial = attend(q_parts, kv_parts, q_starts.astype(jnp.int32), k_starts.astype(jnp.int32))
    pieces = [partial[0]] + [row_shift(partial[k], -k) for k in shifts[1:]]
    levels = [jnp.sum(p[VH : VH + 3].astype(jnp.float32), axis=0, keepdims=True) for p in pieces]
    top = levels[0]
    for level in levels[1:]:
        top = jnp.maximum(top, level)
    shares = [jnp.exp2(level - top) for level in levels]
    merged = sum(w * p[:VH].astype(jnp.float32) for w, p in zip(shares, pieces)) / sum(shares)
    merged = merged.astype(jnp.bfloat16)
    back = row_swap(merged[:, half_len:])
    attended = jnp.concatenate([merged[:, :half_len], back], axis=1)

    tok_count = residual.shape[0]
    token_rows = lax.all_to_all(
        attended.T, "tp", split_axis=0, concat_axis=1, tiled=True
    ).astype(jnp.float32)
    normed_rows = (token_rows * rms_scale(token_rows) * out_gain).astype(jnp.bfloat16)
    mixed = jnp.dot(normed_rows, out_weight, preferred_element_type=jnp.float32)
    middle = residual.astype(jnp.float32) + mixed
    ffn_input = (middle * rms_scale(middle) * ffn_gain).astype(jnp.bfloat16)
    slot_cap = max(2, 9 * tok_count * TOPK // (8 * sp_count))
    slot_total = sp_count * slot_cap
    targets = slot_targets(routes, sp_count, slot_cap)
    chooser = select_matrix(targets, slot_total)
    outbound = (
        jnp.einsum("ts,td->sd", chooser, ffn_input, preferred_element_type=jnp.float32)
        .astype(jnp.bfloat16)
        .reshape(sp_count, slot_cap, D)
    )
    arrived = lax.all_to_all(outbound, "sp", split_axis=0, concat_axis=0, tiled=True)
    my_rows = arrived.reshape(slot_total, D)
    rows = jnp.concatenate([my_rows, core_swap(my_rows)], axis=0)
    hidden = expert_lift(rows, gate_all, up_all)
    sums = expert_lower(hidden, down_all.reshape(-1, D))
    served = (
        sums[:slot_total].astype(jnp.float32)
        + core_swap(sums[slot_total:]).astype(jnp.float32)
    ).astype(jnp.bfloat16)
    returned_rows = lax.all_to_all(
        served.reshape(sp_count, slot_cap, D), "sp", split_axis=0, concat_axis=0, tiled=True
    ).reshape(slot_total, D)
    picked = (
        jnp.take(returned_rows, targets.reshape(-1), axis=0)
        .reshape(tok_count, TOPK, D)
        .astype(jnp.float32)
    )
    moe_sum = jnp.sum(picked * route_weights[:, :, None], axis=1)
    return (middle + moe_sum).astype(jnp.bfloat16)


def solution(mesh):
    return jax.shard_map(
        shards,
        mesh=mesh,
        in_specs=(
            P("sp", "tp"),
            P("sp", None),
            P("sp", None),
            P(),
            P(None, "tp"),
            P(None, "tp"),
            P(),
            P(),
            P(),
            P(),
            P(("sp", "tp"), None),
            P(),
            P(("sp", "tp"), None),
            P(("sp", "tp"), None),
            P("sp", None, "tp"),
            P("sp", None, "tp"),
            P("sp", "tp", None),
        ),
        out_specs=P(("sp", "tp"), None),
        check_vma=False,
    )
```

```python
import jax
import jax.numpy as jnp
from jax import lax
from jax.experimental import pallas as pl
from jax.experimental.pallas import tpu as pltpu
from jax.sharding import PartitionSpec as P

D = 2048
NOPE = 64
ROPE = 32
VH = 64
TOPK = 2
QK = 96
CORES = 2
LANES = 128
TILE = 8
SIDE = 4
LOG2E = 1.4426950408889634
LOW = -1e30


epsilon = 1e-06
rope_base = 10000.0


def rms_scale(values):
    return lax.rsqrt(jnp.mean(values * values, axis=-1, keepdims=True) + epsilon)


def head_prepare(raw, gain_vec, cosine, sine_val):
    scale = lax.rsqrt(jnp.mean(raw * raw, axis=0, keepdims=True) + epsilon)
    normed = raw * scale * gain_vec[:, None]
    first = normed[NOPE : NOPE + ROPE // 2]
    second = normed[NOPE + ROPE // 2 :]
    return jnp.concatenate(
        [normed[:NOPE], first * cosine - second * sine_val, second * cosine + first * sine_val],
        axis=0,
    ).astype(jnp.bfloat16)


def attend_kernel(qs_ref, ks_ref, *refs, tq, tk, parts):
    q_in, kv_in = refs[:parts], refs[parts : 2 * parts]
    out_ref = refs[2 * parts]
    q_buf, kv_buf, k_nat, v_aug, acc, peak, sems = refs[2 * parts + 1 :]
    span = kv_buf.shape[2]
    copies = []
    for i in range(parts):
        for j, (src, dst) in enumerate(((kv_in[i], kv_buf.at[i]), (q_in[i], q_buf.at[i]))):
            copy = pltpu.make_async_copy(src, dst, sems.at[2 * i + j])
            copy.start()
            copies.append(copy)
    for i in range(parts):
        copies[2 * i].wait()
        k_nat[pl.ds(i * span, span), :] = kv_buf[i, :QK, :].astype(jnp.float32).T.astype(jnp.bfloat16)
        for j in range(span // tk):
            piece = i * (span // tk) + j
            v_aug[piece, :VH, :] = kv_buf[i, QK:, j * tk : (j + 1) * tk]
            v_aug[piece, VH:, :] = jnp.ones((16, tk), jnp.bfloat16)
    for i in range(parts):
        copies[2 * i + 1].wait()

    scale = LOG2E * QK ** (-0.5)
    per_q = span // tq
    per_k = span // tk

    def q_tile(t, carry):
        i, h = t // per_q, t % per_q
        q_start = qs_ref[t]
        q = q_buf[i, :, pl.ds(pl.multiple_of(h * tq, tq), tq)]
        acc[...] = jnp.zeros_like(acc)
        peak[...] = jnp.full_like(peak, LOW)

        def k_tile(u, c):
            k_start = ks_ref[u // per_k] + (u % per_k) * tk

            def update(masked):
                keys = k_nat[pl.ds(pl.multiple_of(u * tk, tk), tk), :]
                s = jnp.dot(keys, q, preferred_element_type=jnp.float32) * scale
                if masked:
                    kpos = k_start + lax.broadcasted_iota(jnp.int32, s.shape, 0)
                    qpos = q_start + lax.broadcasted_iota(jnp.int32, s.shape, 1)
                    s = jnp.where(kpos <= qpos, s, LOW)
                old = peak[0:1, :]
                new = jnp.maximum(old, jnp.max(s, axis=0, keepdims=True))
                e = jnp.exp2(s - new).astype(jnp.bfloat16)
                part = jnp.dot(v_aug[u], e, preferred_element_type=jnp.float32)
                acc[...] = acc[...] * jnp.exp2(old - new) + part
                peak[...] = jnp.broadcast_to(new, peak.shape)

            @pl.when(k_start + tk - 1 <= q_start)
            def _():
                update(False)

            @pl.when((k_start + tk - 1 > q_start) & (k_start <= q_start + tq - 1))
            def _():
                update(True)

            return c

        lax.fori_loop(0, parts * per_k, k_tile, 0)
        total = acc[VH : VH + 1, :]
        live = total > 0.0
        safe = jnp.where(live, total, 1.0)
        lse = jnp.where(live, peak[0:1, :] + jnp.log2(safe), LOW)
        hi = lse.astype(jnp.bfloat16)
        mid = (lse - hi.astype(jnp.float32)).astype(jnp.bfloat16)
        lo = (lse - hi.astype(jnp.float32) - mid.astype(jnp.float32)).astype(jnp.bfloat16)
        row = lax.broadcasted_iota(jnp.int32, (16, tq), 0)
        stats = jnp.where(
            row == 0,
            hi.astype(jnp.float32),
            jnp.where(row == 1, mid.astype(jnp.float32), jnp.where(row == 2, lo.astype(jnp.float32), 0.0)),
        )
        cols = pl.ds(pl.multiple_of(h * tq, tq), tq)
        out_ref[i, :VH, cols] = (acc[:VH, :] / safe).astype(jnp.bfloat16)
        out_ref[i, VH:, cols] = stats.astype(jnp.bfloat16)
        return carry

    lax.fori_loop(0, parts * per_q, q_tile, 0)


def attend(q_parts, kv_parts, q_starts, k_starts, tq=512, tk=512):
    parts = len(q_parts)
    span = q_parts[0].shape[1]
    hbm = pl.BlockSpec(memory_space=pl.ANY)
    smem = pl.BlockSpec(memory_space=pltpu.SMEM)

    def kernel(*refs):
        attend_kernel(*refs, tq=tq, tk=tk, parts=parts)

    work = parts * parts * span * span // 2
    return pl.pallas_call(
        kernel,
        out_shape=jax.ShapeDtypeStruct((parts, VH + 16, span), jnp.bfloat16),
        in_specs=[smem, smem] + [hbm] * (2 * parts),
        out_specs=pl.BlockSpec(memory_space=pltpu.VMEM),
        scratch_shapes=[
            pltpu.VMEM((parts, QK, span), jnp.bfloat16),
            pltpu.VMEM((parts, QK + VH, span), jnp.bfloat16),
            pltpu.VMEM((parts * span, QK), jnp.bfloat16),
            pltpu.VMEM((parts * span // tk, VH + 16, tk), jnp.bfloat16),
            pltpu.VMEM((VH + 16, tq), jnp.float32),
            pltpu.VMEM((8, tq), jnp.float32),
            pltpu.SemaphoreType.DMA((2 * parts,)),
        ],
        compiler_params=pltpu.CompilerParams(vmem_limit_bytes=48 * 1024 * 1024),
        cost_estimate=pl.CostEstimate(
            flops=2 * work * (QK + VH), bytes_accessed=3 * 1024 * 1024, transcendentals=work
        ),
        name="attend",
    )(q_starts, k_starts, *q_parts, *kv_parts)


def expert_kernel(x_ref, y_ref, g_ref, u_ref, d_ref, o_ref, p_ref, acc):
    step = pl.program_id(0)
    pairs, _, width = g_ref.shape
    count = x_ref.shape[0]
    rows = jnp.concatenate([x_ref[...], y_ref[...]], axis=0)
    weights = jnp.concatenate(
        [g_ref[i] for i in range(pairs)] + [u_ref[i] for i in range(pairs)], axis=1
    )
    both = jnp.dot(rows, weights, preferred_element_type=jnp.float32)
    half = both.shape[1] // 2
    gate, up = both[:, :half], both[:, half:]
    hidden = (gate / (1.0 + jnp.exp(-gate)) * up).astype(jnp.bfloat16)
    down = jnp.concatenate(
        [
            jnp.concatenate([d_ref[i, j * width : (j + 1) * width, :] for i in range(pairs)], axis=0)
            for j in range(D // LANES)
        ],
        axis=1,
    )
    part = jnp.dot(hidden, down, preferred_element_type=jnp.float32)

    @pl.when(step == 0)
    def _():
        acc[...] = part

    @pl.when(step > 0)
    def _():
        acc[...] += part

    @pl.when(step == pl.num_programs(0) - 1)
    def _():
        o_ref[...] = acc[:count, :].astype(jnp.bfloat16)
        p_ref[...] = acc[count:, :].astype(jnp.bfloat16)


def expert_ffn(rows, others, weights):
    slices, _, width = weights.shape
    pairs = 2
    count = rows.shape[0]
    whole = pl.BlockSpec((count, D), lambda i: (0, 0))
    return pl.pallas_call(
        expert_kernel,
        out_shape=[jax.ShapeDtypeStruct((count, D), jnp.bfloat16)] * 2,
        grid=(slices // pairs,),
        in_specs=[whole, whole]
        + [pl.BlockSpec((pairs, D, width), lambda i, k=k: (i, k, 0)) for k in range(3)],
        out_specs=[whole, whole],
        scratch_shapes=[pltpu.VMEM((2 * count, D), jnp.float32)],
        compiler_params=pltpu.CompilerParams(
            dimension_semantics=("arbitrary",), vmem_limit_bytes=58 * 1024 * 1024
        ),
        cost_estimate=pl.CostEstimate(
            flops=12 * count * D * slices * width,
            bytes_accessed=6 * D * slices * width,
            transcendentals=2 * count * slices * width,
        ),
        name="expert_ffn",
    )(rows, others, weights, weights, weights)


def to_wire(rows, peers):
    tiles = D // LANES
    main = rows[: peers * TILE].reshape(peers, TILE, tiles, LANES)
    main = main.transpose(0, 2, 1, 3).reshape(peers, tiles * TILE, LANES)
    return jnp.concatenate([main, rows[peers * TILE :].reshape(peers, tiles, LANES)], axis=1)


def from_wire(wire):
    peers = wire.shape[0]
    tiles = D // LANES
    main = wire[:, : tiles * TILE].reshape(peers, tiles, TILE, LANES)
    main = main.transpose(0, 2, 1, 3).reshape(peers * TILE, D)
    return jnp.concatenate([main, wire[:, tiles * TILE :].reshape(peers, D)], axis=0)


def slot_targets(route_rows, expert_total):
    flat_routes = route_rows.reshape(-1)
    one_hot = (flat_routes[:, None] == jnp.arange(expert_total, dtype=jnp.int32)[None, :]).astype(
        jnp.int32
    )
    earlier = jnp.cumsum(one_hot, axis=0) - one_hot
    rank_in = jnp.sum(earlier * one_hot, axis=1)
    slots = jnp.where(
        rank_in < TILE, flat_routes * TILE + rank_in, expert_total * TILE + flat_routes
    )
    return slots.reshape(route_rows.shape)


def select_matrix(targets, slot_total):
    hits = targets[:, :, None] == jnp.arange(slot_total, dtype=jnp.int32)[None, None, :]
    return jnp.sum(hits.astype(jnp.bfloat16), axis=1)


def row_shift(value, k):
    pairs = [
        (y * SIDE + x, y * SIDE + (x + k) % SIDE) for y in range(SIDE) for x in range(SIDE)
    ]
    return lax.ppermute(value, "sp", pairs)


def column_shift(value, k):
    pairs = [
        (y * SIDE + x, ((y + k) % SIDE) * SIDE + x) for y in range(SIDE) for x in range(SIDE)
    ]
    return lax.ppermute(value, "sp", pairs)


def row_swap(value):
    pairs = [
        (y * SIDE + x, (SIDE - 1 - y) * SIDE + x) for y in range(SIDE) for x in range(SIDE)
    ]
    return lax.ppermute(value, "sp", pairs)


def expert_exchange(wire):
    return lax.all_to_all(wire, "sp", split_axis=0, concat_axis=0, tiled=True)


def core_swap(value):
    pairs = [(t, t ^ 1) for t in range(lax.axis_size("tp"))]
    return lax.ppermute(value, "tp", pairs)


def shards(
    queries,
    latent,
    rot_key,
    latent_gain,
    key_up,
    value_up,
    query_gain,
    key_gain,
    out_gain,
    out_weight,
    residual,
    ffn_gain,
    routes,
    route_weights,
    expert_gate,
    expert_up,
    expert_down,
):
    shard_len = queries.shape[0]
    half_len = shard_len // 2
    sp_count = lax.axis_size("sp")
    me = lax.axis_index("sp")
    my_y, my_x = me // SIDE, me % SIDE

    same_core = [list(range(c, lax.axis_size("tp"), CORES)) for c in range(CORES)]

    def collect(weights):
        return lax.all_gather(weights, "tp", axis_index_groups=same_core, axis=0, tiled=False)

    down = expert_down[0]
    down = down.reshape(down.shape[0], D // LANES, LANES).transpose(1, 0, 2).reshape(-1, LANES)
    weights = collect(jnp.concatenate([expert_gate[0], expert_up[0], down], axis=0))

    positions = me * shard_len + jnp.arange(shard_len, dtype=jnp.int32)
    inverse = rope_base ** (-jnp.arange(0, ROPE, 2, dtype=jnp.float32) / ROPE)
    angles = positions.astype(jnp.float32)[None, :] * inverse[:, None]
    cosine, sine_val = jnp.cos(angles), jnp.sin(angles)

    query_rows = head_prepare(queries.astype(jnp.float32).T, query_gain, cosine, sine_val)
    swapped = row_swap(query_rows[:, half_len:])
    q_set = jnp.concatenate([query_rows[:, :half_len], swapped], axis=1)

    lat_f32 = latent.astype(jnp.float32)
    normed_latent = (lat_f32 * rms_scale(lat_f32) * latent_gain).astype(jnp.bfloat16)
    both_up = jnp.concatenate([key_up, value_up], axis=1)
    lifted = lax.dot_general(
        both_up, normed_latent, (((0,), (1,)), ((), ())), preferred_element_type=jnp.float32
    ).astype(jnp.bfloat16)
    raw_keys = jnp.concatenate(
        [lifted[:NOPE].astype(jnp.float32), rot_key.astype(jnp.float32).T], axis=0
    )
    bundle = jnp.concatenate(
        [head_prepare(raw_keys, key_gain, cosine, sine_val), lifted[NOPE:]], axis=0
    )

    shifts = range(SIDE)
    kv_parts = [bundle] + [column_shift(bundle, k) for k in shifts[1:]]
    q_parts = [q_set] + [row_shift(q_set, k) for k in shifts[1:]]
    k_starts = jnp.stack([((my_y - k) % SIDE * SIDE + my_x) * shard_len for k in shifts])
    q_cols = [(my_x - k) % SIDE for k in shifts]
    q_starts = jnp.stack(
        sum(
            [
                [
                    (my_y * SIDE + c) * shard_len,
                    ((SIDE - 1 - my_y) * SIDE + c) * shard_len + half_len,
                ]
                for c in q_cols
            ],
            [],
        )
    )
    partial = attend(q_parts, kv_parts, q_starts.astype(jnp.int32), k_starts.astype(jnp.int32))
    pieces = [partial[0]] + [row_shift(partial[k], -k) for k in shifts[1:]]
    levels = [jnp.sum(p[VH : VH + 3].astype(jnp.float32), axis=0, keepdims=True) for p in pieces]
    top = levels[0]
    for level in levels[1:]:
        top = jnp.maximum(top, level)
    factors = [jnp.exp2(level - top) for level in levels]
    merged = sum(w * p[:VH].astype(jnp.float32) for w, p in zip(factors, pieces)) / sum(factors)
    merged = merged.astype(jnp.bfloat16)
    back = row_swap(merged[:, half_len:])
    attended = jnp.concatenate([merged[:, :half_len], back], axis=1)

    tok_count = residual.shape[0]
    token_rows = lax.all_to_all(
        attended.T, "tp", split_axis=0, concat_axis=1, tiled=True
    ).astype(jnp.float32)
    normed_rows = (token_rows * rms_scale(token_rows) * out_gain).astype(jnp.bfloat16)
    mixed = jnp.dot(normed_rows, out_weight, preferred_element_type=jnp.float32)
    middle = residual.astype(jnp.float32) + mixed
    ffn_input = (middle * rms_scale(middle) * ffn_gain).astype(jnp.bfloat16)
    slot_total = sp_count * (TILE + 1)
    targets = slot_targets(routes, sp_count)
    chooser = select_matrix(targets, slot_total)
    outbound = jnp.einsum(
        "ts,td->sd", chooser, ffn_input, preferred_element_type=jnp.float32
    ).astype(jnp.bfloat16)
    my_rows = from_wire(expert_exchange(to_wire(outbound, sp_count)))
    own_sum, other_sum = expert_ffn(my_rows, core_swap(my_rows), weights)
    served = (
        own_sum.astype(jnp.float32) + core_swap(other_sum).astype(jnp.float32)
    ).astype(jnp.bfloat16)
    returned_rows = from_wire(expert_exchange(to_wire(served, sp_count)))
    hits = targets[:, :, None] == jnp.arange(slot_total, dtype=jnp.int32)[None, None, :]
    shares = jnp.sum(jnp.where(hits, route_weights[:, :, None], 0.0), axis=1)
    moe_sum = jnp.dot(
        shares,
        returned_rows.astype(jnp.float32),
        precision=lax.Precision.HIGHEST,
        preferred_element_type=jnp.float32,
    )
    return (middle + moe_sum).astype(jnp.bfloat16)


def solution(mesh):
    return jax.shard_map(
        shards,
        mesh=mesh,
        in_specs=(
            P("sp", "tp"),
            P("sp", None),
            P("sp", None),
            P(),
            P(None, "tp"),
            P(None, "tp"),
            P(),
            P(),
            P(),
            P(),
            P(("sp", "tp"), None),
            P(),
            P(("sp", "tp"), None),
            P(("sp", "tp"), None),
            P("sp", None, "tp"),
            P("sp", None, "tp"),
            P("sp", "tp", None),
        ),
        out_specs=P(("sp", "tp"), None),
        check_vma=False,
    )
```

```python
import jax
import jax.numpy as jnp
from jax import lax
from jax.experimental import pallas as pl
from jax.experimental.pallas import tpu as pltpu
from jax.sharding import PartitionSpec as P


D = 2048
NOPE = 64
ROPE = 32
VH = 64
QK = 96
CORES = 2
LANES = 128
TILE = 8
SIDE = 4
LOG2E = 1.4426950408889634
LOW = -1e30


epsilon = 1e-06
rope_base = 10000.0


def rms_scale(values):
    return lax.rsqrt(jnp.mean(values * values, axis=-1, keepdims=True) + epsilon)


def head_prepare(raw, gain_vec, cosine, sine_val):
    scale = lax.rsqrt(jnp.mean(raw * raw, axis=0, keepdims=True) + epsilon)
    normed = raw * scale * gain_vec[:, None]
    first = normed[NOPE : NOPE + ROPE // 2]
    second = normed[NOPE + ROPE // 2 :]
    return jnp.concatenate(
        [normed[:NOPE], first * cosine - second * sine_val, second * cosine + first * sine_val],
        axis=0,
    ).astype(jnp.bfloat16)


def attend_kernel(qs_ref, ks_ref, *refs, tq, tk, kb, parts):
    q_in, kv_in = refs[:parts], refs[parts : 2 * parts]
    out_ref = refs[2 * parts]
    q_buf, kv_buf, k_nat, v_aug, acc, peak, sems = refs[2 * parts + 1 :]
    span = kv_buf.shape[2]
    copies = []
    for i in range(parts):
        for j, (src, dst) in enumerate(((kv_in[i], kv_buf.at[i]), (q_in[i], q_buf.at[i]))):
            copy = pltpu.make_async_copy(src, dst, sems.at[2 * i + j])
            copy.start()
            copies.append(copy)
    for i in range(parts):
        copies[2 * i].wait()
        k_nat[pl.ds(i * span, span), :] = kv_buf[i, :QK, :].T
        for j in range(span // tk):
            piece = i * (span // tk) + j
            v_aug[piece, :VH, :] = kv_buf[i, QK:, j * tk : (j + 1) * tk]
            v_aug[piece, VH:, :] = jnp.ones((16, tk), jnp.bfloat16)
    for i in range(parts):
        copies[2 * i + 1].wait()

    scale = LOG2E * QK ** (-0.5)
    per_q = span // tq
    per_k = span // tk

    def q_tile(t, carry):
        i, h = t // per_q, t % per_q
        q_start = qs_ref[t]
        q = q_buf[i, :, pl.ds(pl.multiple_of(h * tq, tq), tq)]
        acc[...] = jnp.zeros_like(acc)
        peak[...] = jnp.full_like(peak, LOW)

        def k_tile(u, c):
            k_start = ks_ref[u // per_k] + (u % per_k) * tk

            def score(r, masked):
                keys = k_nat[pl.ds(pl.multiple_of(u * tk + r * kb, kb), kb), :]
                s = jnp.dot(keys, q, preferred_element_type=jnp.float32)
                if masked:
                    kpos = k_start + r * kb + lax.broadcasted_iota(jnp.int32, s.shape, 0)
                    qpos = q_start + lax.broadcasted_iota(jnp.int32, s.shape, 1)
                    s = jnp.where(kpos <= qpos, s, LOW)
                return s

            def update(masked):
                old, total = peak[0:1, :], acc[...]
                ahead = score(0, masked)
                for r in range(tk // kb):
                    s = ahead
                    if (r + 1) * kb < tk:
                        ahead = score(r + 1, masked)
                    new = jnp.maximum(old, jnp.max(s, axis=0, keepdims=True))
                    e = jnp.exp2((s - new) * scale).astype(jnp.bfloat16)
                    part = jnp.dot(
                        v_aug[u, :, r * kb : (r + 1) * kb], e, preferred_element_type=jnp.float32
                    )
                    total = total * jnp.exp2((old - new) * scale) + part
                    old = new
                acc[...] = total
                peak[...] = jnp.broadcast_to(old, peak.shape)

            @pl.when(k_start + tk - 1 <= q_start)
            def _():
                update(False)

            @pl.when((k_start + tk - 1 > q_start) & (k_start <= q_start + tq - 1))
            def _():
                update(True)

            return c

        lax.fori_loop(0, parts * per_k, k_tile, 0)
        total = acc[VH : VH + 1, :]
        live = total > 0.0
        safe = jnp.where(live, total, 1.0)
        lse = jnp.where(live, peak[0:1, :] * scale + jnp.log2(safe), LOW)
        hi = lse.astype(jnp.bfloat16)
        mid = (lse - hi.astype(jnp.float32)).astype(jnp.bfloat16)
        lo = (lse - hi.astype(jnp.float32) - mid.astype(jnp.float32)).astype(jnp.bfloat16)
        row = lax.broadcasted_iota(jnp.int32, (16, tq), 0)
        stats = jnp.where(
            row == 0,
            hi.astype(jnp.float32),
            jnp.where(row == 1, mid.astype(jnp.float32), jnp.where(row == 2, lo.astype(jnp.float32), 0.0)),
        )
        cols = pl.ds(pl.multiple_of(h * tq, tq), tq)
        out_ref[i, :VH, cols] = (acc[:VH, :] / safe).astype(jnp.bfloat16)
        out_ref[i, VH:, cols] = stats.astype(jnp.bfloat16)
        return carry

    lax.fori_loop(0, parts * per_q, q_tile, 0)


def attend(q_parts, kv_parts, q_starts, k_starts, tq=512, tk=1024, kb=512):
    parts = len(q_parts)
    span = q_parts[0].shape[1]
    hbm = pl.BlockSpec(memory_space=pltpu.HBM)
    smem = pl.BlockSpec(memory_space=pltpu.SMEM)

    def kernel(*refs):
        attend_kernel(*refs, tq=tq, tk=tk, kb=kb, parts=parts)

    work = parts * parts * span * span // 2
    return pl.pallas_call(
        kernel,
        out_shape=jax.ShapeDtypeStruct((parts, VH + 16, span), jnp.bfloat16),
        in_specs=[smem, smem] + [hbm] * (2 * parts),
        out_specs=pl.BlockSpec(memory_space=pltpu.VMEM),
        scratch_shapes=[
            pltpu.VMEM((parts, QK, span), jnp.bfloat16),
            pltpu.VMEM((parts, QK + VH, span), jnp.bfloat16),
            pltpu.VMEM((parts * span, QK), jnp.bfloat16),
            pltpu.VMEM((parts * span // tk, VH + 16, tk), jnp.bfloat16),
            pltpu.VMEM((VH + 16, tq), jnp.float32),
            pltpu.VMEM((8, tq), jnp.float32),
            pltpu.SemaphoreType.DMA((2 * parts,)),
        ],
        compiler_params=pltpu.CompilerParams(vmem_limit_bytes=60 * 1024 * 1024),
        cost_estimate=pl.CostEstimate(
            flops=2 * work * (QK + VH), bytes_accessed=3 * 1024 * 1024, transcendentals=work
        ),
        name="attend",
    )(q_starts, k_starts, *q_parts, *kv_parts)


def expert_group(rows, w_buf, slots):
    width = w_buf.shape[2]
    weights = jnp.concatenate(
        [w_buf[s, :D, :] for s in slots] + [w_buf[s, D : 2 * D, :] for s in slots], axis=1
    )
    both = jnp.dot(rows, weights, preferred_element_type=jnp.float32)
    half = both.shape[1] // 2
    gate, up = both[:, :half], both[:, half:]
    hidden = (gate / (1.0 + jnp.exp(-gate)) * up).astype(jnp.bfloat16)
    down = jnp.concatenate(
        [
            jnp.concatenate(
                [w_buf[s, 2 * D + j * width : 2 * D + (j + 1) * width, :] for s in slots], axis=0
            )
            for j in range(D // LANES)
        ],
        axis=1,
    )
    return jnp.dot(hidden, down, preferred_element_type=jnp.float32)


def expert_kernel(*refs, places, pairs, adds, ends):
    total = len(places)
    x_ref, y_ref = refs[:2]
    before, refs = refs[2 : 2 + adds], refs[2 + adds :]
    w_refs, refs = refs[:total], refs[total:]
    outs, (acc, w_buf, sems) = refs[:-3], refs[-3:]
    copies = [
        pltpu.make_async_copy(w_refs[i], w_buf.at[s, pl.ds(first, size)], sems.at[i])
        for i, (s, first, size) in enumerate(places)
    ]
    for copy in copies:
        copy.start()
    rows = jnp.concatenate([x_ref[...], y_ref[...]], axis=0)
    slices = w_buf.shape[0]
    first = 0
    while first < slices:
        slots = list(range(first, min(slices, first + (pairs if slices % pairs == 0 or first else 1))))
        for copy, place in zip(copies, places):
            if place[0] in slots:
                copy.wait()
        part = expert_group(rows, w_buf, slots)
        if first:
            part = acc[...] + part
        elif adds:
            part = before[0][...] + part
        acc[...] = part
        first = slots[-1] + 1
    if ends:
        count = x_ref.shape[0]
        outs[0][...] = acc[:count, :].astype(jnp.bfloat16)
        outs[1][...] = acc[count:, :].astype(jnp.bfloat16)
    else:
        outs[0][...] = acc[...]


def expert_ffn(rows, others, before, pieces, places, ends):
    count = rows.shape[0]
    slices, depth, width = 1 + max(p[0] for p in places), 3 * D, LANES
    vmem = pl.BlockSpec(memory_space=pltpu.VMEM)
    hbm = pl.BlockSpec(memory_space=pltpu.HBM)
    if ends:
        outs = [jax.ShapeDtypeStruct((count, D), jnp.bfloat16)] * 2
    else:
        outs = [jax.ShapeDtypeStruct((2 * count, D), jnp.float32)]

    def kernel(*refs):
        expert_kernel(*refs, places=places, pairs=2, adds=len(before), ends=ends)

    return pl.pallas_call(
        kernel,
        out_shape=outs,
        in_specs=[vmem, vmem] + [vmem] * len(before) + [hbm] * len(pieces),
        out_specs=[vmem] * len(outs),
        scratch_shapes=[
            pltpu.VMEM((2 * count, D), jnp.float32),
            pltpu.VMEM((slices, depth, width), jnp.bfloat16),
            pltpu.SemaphoreType.DMA((len(pieces),)),
        ],
        compiler_params=pltpu.CompilerParams(vmem_limit_bytes=58 * 1024 * 1024),
        cost_estimate=pl.CostEstimate(
            flops=12 * count * D * slices * width,
            bytes_accessed=6 * D * slices * width,
            transcendentals=2 * count * slices * width,
        ),
    )(rows, others, *before, *pieces)


def to_wire(rows, peers):
    tiles = D // LANES
    main = rows[: peers * TILE].reshape(peers, TILE, tiles, LANES)
    main = main.transpose(0, 2, 1, 3).reshape(peers, tiles * TILE, LANES)
    return jnp.concatenate([main, rows[peers * TILE :].reshape(peers, tiles, LANES)], axis=1)


def from_wire(wire):
    peers = wire.shape[0]
    tiles = D // LANES
    main = wire[:, : tiles * TILE].reshape(peers, tiles, TILE, LANES)
    main = main.transpose(0, 2, 1, 3).reshape(peers * TILE, D)
    return jnp.concatenate([main, wire[:, tiles * TILE :].reshape(peers, D)], axis=0)


def slot_targets(route_rows, expert_total):
    flat_routes = route_rows.reshape(-1)
    one_hot = (flat_routes[:, None] == jnp.arange(expert_total, dtype=jnp.int32)[None, :]).astype(
        jnp.int32
    )
    earlier = jnp.cumsum(one_hot, axis=0) - one_hot
    rank_in = jnp.sum(earlier * one_hot, axis=1)
    slots = jnp.where(
        rank_in < TILE, flat_routes * TILE + rank_in, expert_total * TILE + flat_routes
    )
    return slots.reshape(route_rows.shape)


def select_matrix(targets, slot_total):
    hits = targets[:, :, None] == jnp.arange(slot_total, dtype=jnp.int32)[None, None, :]
    return jnp.sum(hits.astype(jnp.bfloat16), axis=1)


def row_shift(value, k):
    pairs = [
        (y * SIDE + x, y * SIDE + (x + k) % SIDE) for y in range(SIDE) for x in range(SIDE)
    ]
    return lax.ppermute(value, "sp", pairs)


def column_shift(value, k):
    pairs = [
        (y * SIDE + x, ((y + k) % SIDE) * SIDE + x) for y in range(SIDE) for x in range(SIDE)
    ]
    return lax.ppermute(value, "sp", pairs)


def row_swap(value):
    pairs = [
        (y * SIDE + x, (SIDE - 1 - y) * SIDE + x) for y in range(SIDE) for x in range(SIDE)
    ]
    return lax.ppermute(value, "sp", pairs)


def expert_exchange(wire):
    return lax.all_to_all(wire, "sp", split_axis=0, concat_axis=0, tiled=True)


def z_shift(value, k):
    count = lax.axis_size("tp")
    return lax.ppermute(value, "tp", [(t, (t + CORES * k) % count) for t in range(count)])


def core_swap(value):
    pairs = [(t, t ^ 1) for t in range(lax.axis_size("tp"))]
    return lax.ppermute(value, "tp", pairs)


def shards(
    queries,
    latent,
    rot_key,
    latent_gain,
    key_up,
    value_up,
    query_gain,
    key_gain,
    out_gain,
    out_weight,
    residual,
    ffn_gain,
    routes,
    route_weights,
    expert_gate,
    expert_up,
    expert_down,
):
    shard_len = queries.shape[0]
    half_len = shard_len // 2
    sp_count = lax.axis_size("sp")
    me = lax.axis_index("sp")
    my_y, my_x = me // SIDE, me % SIDE

    gate, up, down = expert_gate[0], expert_up[0], expert_down[0]
    down = down.reshape(down.shape[0], D // LANES, LANES).transpose(1, 0, 2).reshape(-1, LANES)
    halves = [
        jnp.concatenate([gate, up[: D // 2]], axis=0),
        jnp.concatenate([up[D // 2 :], down], axis=0),
    ]
    ahead, behind = [[half] for half in halves], [[half] for half in halves]

    def ring_step(h, n):
        front, back = ahead[h][-1], behind[h][-1]
        if n < 4 or h == 0:
            ahead[h].append(z_shift(front, 1))
        if n < 4 or h == 1:
            behind[h].append(z_shift(back, -1))

    for n in (1, 2, 3, 4):
        for h in (0, 1):
            ring_step(h, n)

    positions = me * shard_len + jnp.arange(shard_len, dtype=jnp.int32)
    inverse = rope_base ** (-jnp.arange(0, ROPE, 2, dtype=jnp.float32) / ROPE)
    angles = positions.astype(jnp.float32)[None, :] * inverse[:, None]
    cosine, sine_val = jnp.cos(angles), jnp.sin(angles)

    query_rows = head_prepare(queries.astype(jnp.float32).T, query_gain, cosine, sine_val)
    swapped = row_swap(query_rows[:, half_len:])
    q_set = jnp.concatenate([query_rows[:, :half_len], swapped], axis=1)

    lat_f32 = latent.astype(jnp.float32)
    normed_latent = (lat_f32 * rms_scale(lat_f32) * latent_gain).astype(jnp.bfloat16)
    both_up = jnp.concatenate([key_up, value_up], axis=1)
    lifted = lax.dot_general(
        both_up, normed_latent, (((0,), (1,)), ((), ())), preferred_element_type=jnp.float32
    ).astype(jnp.bfloat16)
    raw_keys = jnp.concatenate(
        [lifted[:NOPE].astype(jnp.float32), rot_key.astype(jnp.float32).T], axis=0
    )
    bundle = jnp.concatenate(
        [head_prepare(raw_keys, key_gain, cosine, sine_val), lifted[NOPE:]], axis=0
    )

    shifts = range(SIDE)
    kv_parts = [bundle] + [column_shift(bundle, k) for k in shifts[1:]]
    q_parts = [q_set] + [row_shift(q_set, k) for k in shifts[1:]]
    k_starts = jnp.stack([((my_y - k) % SIDE * SIDE + my_x) * shard_len for k in shifts])
    q_cols = [(my_x - k) % SIDE for k in shifts]
    q_starts = jnp.stack(
        sum(
            [
                [
                    (my_y * SIDE + c) * shard_len,
                    ((SIDE - 1 - my_y) * SIDE + c) * shard_len + half_len,
                ]
                for c in q_cols
            ],
            [],
        )
    )
    partial = attend(q_parts, kv_parts, q_starts.astype(jnp.int32), k_starts.astype(jnp.int32))
    pieces = [partial[0]] + [row_shift(partial[k], -k) for k in shifts[1:]]
    levels = [jnp.sum(p[VH : VH + 3].astype(jnp.float32), axis=0, keepdims=True) for p in pieces]
    top = levels[0]
    for level in levels[1:]:
        top = jnp.maximum(top, level)
    factors = [jnp.exp2(level - top) for level in levels]
    merged = sum(w * p[:VH].astype(jnp.float32) for w, p in zip(factors, pieces)) / sum(factors)
    merged = merged.astype(jnp.bfloat16)
    back = row_swap(merged[:, half_len:])
    attended = jnp.concatenate([merged[:, :half_len], back], axis=1)

    token_rows = lax.all_to_all(attended.T, "tp", split_axis=0, concat_axis=1, tiled=True)
    token_rows = token_rows.astype(jnp.float32)
    normed_rows = (token_rows * rms_scale(token_rows) * out_gain).astype(jnp.bfloat16)
    mixed = jnp.dot(normed_rows, out_weight, preferred_element_type=jnp.float32)
    middle = residual.astype(jnp.float32) + mixed
    ffn_input = (middle * rms_scale(middle) * ffn_gain).astype(jnp.bfloat16)
    slot_total = sp_count * (TILE + 1)
    targets = slot_targets(routes, sp_count)
    chooser = select_matrix(targets, slot_total)
    outbound = jnp.einsum(
        "ts,td->sd", chooser, ffn_input, preferred_element_type=jnp.float32
    ).astype(jnp.bfloat16)
    arrived = expert_exchange(to_wire(outbound, sp_count))
    my_rows = from_wire(arrived)
    their_rows = core_swap(my_rows)
    weight_pieces, places = [], []
    for h, half in enumerate(halves):
        size = half.shape[0]
        start = h * size
        for n in range(4):
            for way, ring in ((0, ahead[h]), (1, behind[h])):
                if n == 0 and way == 1:
                    continue
                weight_pieces.append(ring[n])
                places.append((2 * n - 1 + way if n else 0, start, size))
    first_sum = expert_ffn(my_rows, their_rows, [], weight_pieces, places, False)
    last_pieces = [ahead[0][4], behind[1][4]]
    size = halves[0].shape[0]
    last_places = [(0, 0, size), (0, size, size)]
    own_sum, other_sum = expert_ffn(my_rows, their_rows, first_sum, last_pieces, last_places, True)
    served = (
        own_sum.astype(jnp.float32) + core_swap(other_sum).astype(jnp.float32)
    ).astype(jnp.bfloat16)
    returned_rows = from_wire(expert_exchange(to_wire(served, sp_count)))
    hits = targets[:, :, None] == jnp.arange(slot_total, dtype=jnp.int32)[None, None, :]
    shares = jnp.sum(jnp.where(hits, route_weights[:, :, None], 0.0), axis=1)
    moe_sum = jnp.dot(
        shares,
        returned_rows.astype(jnp.float32),
        precision=lax.Precision.HIGHEST,
        preferred_element_type=jnp.float32,
    )
    return (middle + moe_sum).astype(jnp.bfloat16)


def solution(mesh):
    return jax.shard_map(
        shards,
        mesh=mesh,
        in_specs=(
            P("sp", "tp"),
            P("sp", None),
            P("sp", None),
            P(),
            P(None, "tp"),
            P(None, "tp"),
            P(),
            P(),
            P(),
            P(),
            P(("sp", "tp"), None),
            P(),
            P(("sp", "tp"), None),
            P(("sp", "tp"), None),
            P("sp", None, "tp"),
            P("sp", None, "tp"),
            P("sp", "tp", None),
        ),
        out_specs=P(("sp", "tp"), None),
        check_vma=False,
    )
```

```python
import jax
import jax.numpy as jnp
from jax import lax
from jax.experimental import pallas as pl
from jax.experimental.pallas import tpu as pltpu
from jax.sharding import PartitionSpec as P


D = 2048
NOPE = 64
ROPE = 32
VH = 64
QK = 96
CORES = 2
LANES = 128
TILE = 8
SIDE = 4
LOG2E = 1.4426950408889634
LOW = -1e30


epsilon = 1e-06
rope_base = 10000.0


def rms_scale(values):
    return lax.rsqrt(jnp.mean(values * values, axis=-1, keepdims=True) + epsilon)


def head_prepare(raw, gain_vec, cosine, sine_val):
    scale = lax.rsqrt(jnp.mean(raw * raw, axis=0, keepdims=True) + epsilon)
    normed = raw * scale * gain_vec[:, None]
    first = normed[NOPE : NOPE + ROPE // 2]
    second = normed[NOPE + ROPE // 2 :]
    return jnp.concatenate(
        [normed[:NOPE], first * cosine - second * sine_val, second * cosine + first * sine_val],
        axis=0,
    ).astype(jnp.bfloat16)


def attend_kernel(qs_ref, ks_ref, *refs, tq, tk, kb, parts):
    q_in, kv_in = refs[:parts], refs[parts : 2 * parts]
    out_ref = refs[2 * parts]
    q_buf, kv_buf, k_nat, v_aug, acc, peak, sems = refs[2 * parts + 1 :]
    span = kv_buf.shape[2]
    copies = []
    for i in range(parts):
        for j, (src, dst) in enumerate(((kv_in[i], kv_buf.at[i]), (q_in[i], q_buf.at[i]))):
            copy = pltpu.make_async_copy(src, dst, sems.at[2 * i + j])
            copy.start()
            copies.append(copy)
    for i in range(parts):
        copies[2 * i].wait()
        k_nat[pl.ds(i * span, span), :] = kv_buf[i, :QK, :].T
        for j in range(span // tk):
            piece = i * (span // tk) + j
            v_aug[piece, :VH, :] = kv_buf[i, QK:, j * tk : (j + 1) * tk]
            v_aug[piece, VH:, :] = jnp.ones((16, tk), jnp.bfloat16)
    for i in range(parts):
        copies[2 * i + 1].wait()

    scale = LOG2E * QK ** (-0.5)
    per_q = span // tq
    per_k = span // tk

    def q_tile(t, carry):
        i, h = t // per_q, t % per_q
        q_start = qs_ref[t]
        q = q_buf[i, :, pl.ds(pl.multiple_of(h * tq, tq), tq)]
        acc[...] = jnp.zeros_like(acc)
        peak[...] = jnp.full_like(peak, LOW)

        def k_tile(u, c):
            k_start = ks_ref[u // per_k] + (u % per_k) * tk

            def score(r, masked):
                keys = k_nat[pl.ds(pl.multiple_of(u * tk + r * kb, kb), kb), :]
                s = jnp.dot(keys, q, preferred_element_type=jnp.float32)
                if masked:
                    kpos = k_start + r * kb + lax.broadcasted_iota(jnp.int32, s.shape, 0)
                    qpos = q_start + lax.broadcasted_iota(jnp.int32, s.shape, 1)
                    s = jnp.where(kpos <= qpos, s, LOW)
                return s

            def update(masked):
                old, total = peak[0:1, :], acc[...]
                ahead = score(0, masked)
                for r in range(tk // kb):
                    s = ahead
                    if (r + 1) * kb < tk:
                        ahead = score(r + 1, masked)
                    new = jnp.maximum(old, jnp.max(s, axis=0, keepdims=True))
                    e = jnp.exp2((s - new) * scale).astype(jnp.bfloat16)
                    part = jnp.dot(
                        v_aug[u, :, r * kb : (r + 1) * kb], e, preferred_element_type=jnp.float32
                    )
                    total = total * jnp.exp2((old - new) * scale) + part
                    old = new
                acc[...] = total
                peak[...] = jnp.broadcast_to(old, peak.shape)

            @pl.when(k_start + tk - 1 <= q_start)
            def _():
                update(False)

            @pl.when((k_start + tk - 1 > q_start) & (k_start <= q_start + tq - 1))
            def _():
                update(True)

            return c

        lax.fori_loop(0, parts * per_k, k_tile, 0)
        total = acc[VH : VH + 1, :]
        live = total > 0.0
        safe = jnp.where(live, total, 1.0)
        lse = jnp.where(live, peak[0:1, :] * scale + jnp.log2(safe), LOW)
        hi = lse.astype(jnp.bfloat16)
        mid = (lse - hi.astype(jnp.float32)).astype(jnp.bfloat16)
        lo = (lse - hi.astype(jnp.float32) - mid.astype(jnp.float32)).astype(jnp.bfloat16)
        row = lax.broadcasted_iota(jnp.int32, (16, tq), 0)
        stats = jnp.where(
            row == 0,
            hi.astype(jnp.float32),
            jnp.where(row == 1, mid.astype(jnp.float32), jnp.where(row == 2, lo.astype(jnp.float32), 0.0)),
        )
        cols = pl.ds(pl.multiple_of(h * tq, tq), tq)
        out_ref[i, :VH, cols] = (acc[:VH, :] / safe).astype(jnp.bfloat16)
        out_ref[i, VH:, cols] = stats.astype(jnp.bfloat16)
        return carry

    lax.fori_loop(0, parts * per_q, q_tile, 0)


def attend(q_parts, kv_parts, q_starts, k_starts, tq=512, tk=1024, kb=512):
    parts = len(q_parts)
    span = q_parts[0].shape[1]
    hbm = pl.BlockSpec(memory_space=pltpu.HBM)
    smem = pl.BlockSpec(memory_space=pltpu.SMEM)

    def kernel(*refs):
        attend_kernel(*refs, tq=tq, tk=tk, kb=kb, parts=parts)

    work = parts * parts * span * span // 2
    return pl.pallas_call(
        kernel,
        out_shape=jax.ShapeDtypeStruct((parts, VH + 16, span), jnp.bfloat16),
        in_specs=[smem, smem] + [hbm] * (2 * parts),
        out_specs=pl.BlockSpec(memory_space=pltpu.VMEM),
        scratch_shapes=[
            pltpu.VMEM((parts, QK, span), jnp.bfloat16),
            pltpu.VMEM((parts, QK + VH, span), jnp.bfloat16),
            pltpu.VMEM((parts * span, QK), jnp.bfloat16),
            pltpu.VMEM((parts * span // tk, VH + 16, tk), jnp.bfloat16),
            pltpu.VMEM((VH + 16, tq), jnp.float32),
            pltpu.VMEM((8, tq), jnp.float32),
            pltpu.SemaphoreType.DMA((2 * parts,)),
        ],
        compiler_params=pltpu.CompilerParams(vmem_limit_bytes=60 * 1024 * 1024),
        cost_estimate=pl.CostEstimate(
            flops=2 * work * (QK + VH), bytes_accessed=3 * 1024 * 1024, transcendentals=work
        ),
        name="attend",
    )(q_starts, k_starts, *q_parts, *kv_parts)


def expert_group(rows, w_buf, slots):
    width = w_buf.shape[2]
    weights = jnp.concatenate(
        [w_buf[s, :D, :] for s in slots] + [w_buf[s, D : 2 * D, :] for s in slots], axis=1
    )
    both = jnp.dot(rows, weights, preferred_element_type=jnp.float32)
    half = both.shape[1] // 2
    gate, up = both[:, :half], both[:, half:]
    hidden = (gate / (1.0 + jnp.exp(-gate)) * up).astype(jnp.bfloat16)
    down = jnp.concatenate(
        [
            jnp.concatenate(
                [w_buf[s, 2 * D + j * width : 2 * D + (j + 1) * width, :] for s in slots], axis=0
            )
            for j in range(D // LANES)
        ],
        axis=1,
    )
    return jnp.dot(hidden, down, preferred_element_type=jnp.float32)


def expert_kernel(x_ref, y_ref, *refs, places, pairs):
    total = len(places)
    w_refs, (o_ref, p_ref, acc, w_buf, sems) = refs[:total], refs[total:]
    copies = [
        pltpu.make_async_copy(w_refs[i], w_buf.at[s, pl.ds(first, size)], sems.at[i])
        for i, (s, first, size) in enumerate(places)
    ]
    for copy in copies:
        copy.start()
    rows = jnp.concatenate([x_ref[...], y_ref[...]], axis=0)
    slices = w_buf.shape[0]
    for first in range(0, slices, pairs):
        slots = list(range(first, first + pairs))
        for copy, place in zip(copies, places):
            if place[0] in slots:
                copy.wait()
        part = expert_group(rows, w_buf, slots)
        acc[...] = part if first == 0 else acc[...] + part
    count = x_ref.shape[0]
    o_ref[...] = acc[:count, :].astype(jnp.bfloat16)
    p_ref[...] = acc[count:, :].astype(jnp.bfloat16)


def expert_ffn(rows, others, pieces, places):
    count = rows.shape[0]
    slices, depth, width = 1 + max(p[0] for p in places), 3 * D, LANES
    vmem = pl.BlockSpec(memory_space=pltpu.VMEM)
    hbm = pl.BlockSpec(memory_space=pl.ANY)

    def kernel(*refs):
        expert_kernel(*refs, places=places, pairs=2)

    return pl.pallas_call(
        kernel,
        out_shape=[jax.ShapeDtypeStruct((count, D), jnp.bfloat16)] * 2,
        in_specs=[vmem, vmem] + [hbm] * len(pieces),
        out_specs=[vmem, vmem],
        scratch_shapes=[
            pltpu.VMEM((2 * count, D), jnp.float32),
            pltpu.VMEM((slices, depth, width), jnp.bfloat16),
            pltpu.SemaphoreType.DMA((len(pieces),)),
        ],
        compiler_params=pltpu.CompilerParams(vmem_limit_bytes=34 * 1024 * 1024),
        cost_estimate=pl.CostEstimate(
            flops=12 * count * D * slices * width,
            bytes_accessed=6 * D * slices * width,
            transcendentals=2 * count * slices * width,
        ),
        name="expert_ffn",
    )(rows, others, *pieces)


def to_wire(rows, peers):
    tiles = D // LANES
    main = rows[: peers * TILE].reshape(peers, TILE, tiles, LANES)
    main = main.transpose(0, 2, 1, 3).reshape(peers, tiles * TILE, LANES)
    return jnp.concatenate([main, rows[peers * TILE :].reshape(peers, tiles, LANES)], axis=1)


def from_wire(wire):
    peers = wire.shape[0]
    tiles = D // LANES
    main = wire[:, : tiles * TILE].reshape(peers, tiles, TILE, LANES)
    main = main.transpose(0, 2, 1, 3).reshape(peers * TILE, D)
    return jnp.concatenate([main, wire[:, tiles * TILE :].reshape(peers, D)], axis=0)


def slot_targets(route_rows, expert_total):
    flat_routes = route_rows.reshape(-1)
    one_hot = (flat_routes[:, None] == jnp.arange(expert_total, dtype=jnp.int32)[None, :]).astype(
        jnp.int32
    )
    earlier = jnp.cumsum(one_hot, axis=0) - one_hot
    rank_in = jnp.sum(earlier * one_hot, axis=1)
    slots = jnp.where(
        rank_in < TILE, flat_routes * TILE + rank_in, expert_total * TILE + flat_routes
    )
    return slots.reshape(route_rows.shape)


def select_matrix(targets, slot_total):
    hits = targets[:, :, None] == jnp.arange(slot_total, dtype=jnp.int32)[None, None, :]
    return jnp.sum(hits.astype(jnp.bfloat16), axis=1)


def row_shift(value, k):
    pairs = [
        (y * SIDE + x, y * SIDE + (x + k) % SIDE) for y in range(SIDE) for x in range(SIDE)
    ]
    return lax.ppermute(value, "sp", pairs)


def column_shift(value, k):
    pairs = [
        (y * SIDE + x, ((y + k) % SIDE) * SIDE + x) for y in range(SIDE) for x in range(SIDE)
    ]
    return lax.ppermute(value, "sp", pairs)


def row_swap(value):
    pairs = [
        (y * SIDE + x, (SIDE - 1 - y) * SIDE + x) for y in range(SIDE) for x in range(SIDE)
    ]
    return lax.ppermute(value, "sp", pairs)


def expert_exchange(wire):
    return lax.all_to_all(wire, "sp", split_axis=0, concat_axis=0, tiled=True)


def z_shift(value, k):
    count = lax.axis_size("tp")
    return lax.ppermute(value, "tp", [(t, (t + CORES * k) % count) for t in range(count)])


def core_swap(value):
    pairs = [(t, t ^ 1) for t in range(lax.axis_size("tp"))]
    return lax.ppermute(value, "tp", pairs)


def shards(
    queries,
    latent,
    rot_key,
    latent_gain,
    key_up,
    value_up,
    query_gain,
    key_gain,
    out_gain,
    out_weight,
    residual,
    ffn_gain,
    routes,
    route_weights,
    expert_gate,
    expert_up,
    expert_down,
):
    shard_len = queries.shape[0]
    half_len = shard_len // 2
    sp_count = lax.axis_size("sp")
    me = lax.axis_index("sp")
    my_y, my_x = me // SIDE, me % SIDE

    gate, up, down = expert_gate[0], expert_up[0], expert_down[0]
    down = down.reshape(down.shape[0], D // LANES, LANES).transpose(1, 0, 2).reshape(-1, LANES)
    halves = [
        jnp.concatenate([gate, up[: D // 2]], axis=0),
        jnp.concatenate([up[D // 2 :], down], axis=0),
    ]
    ahead, behind = [[half] for half in halves], [[half] for half in halves]

    def ring_step(h, n):
        front, back = ahead[h][-1], behind[h][-1]
        if n < 4 or h == 0:
            ahead[h].append(z_shift(front, 1))
        if n < 4 or h == 1:
            behind[h].append(z_shift(back, -1))

    for n in (1, 2, 3, 4):
        for h in (0, 1):
            ring_step(h, n)

    positions = me * shard_len + jnp.arange(shard_len, dtype=jnp.int32)
    inverse = rope_base ** (-jnp.arange(0, ROPE, 2, dtype=jnp.float32) / ROPE)
    angles = positions.astype(jnp.float32)[None, :] * inverse[:, None]
    cosine, sine_val = jnp.cos(angles), jnp.sin(angles)

    query_rows = head_prepare(queries.astype(jnp.float32).T, query_gain, cosine, sine_val)
    swapped = row_swap(query_rows[:, half_len:])
    q_set = jnp.concatenate([query_rows[:, :half_len], swapped], axis=1)

    lat_f32 = latent.astype(jnp.float32)
    normed_latent = (lat_f32 * rms_scale(lat_f32) * latent_gain).astype(jnp.bfloat16)
    both_up = jnp.concatenate([key_up, value_up], axis=1)
    lifted = lax.dot_general(
        both_up, normed_latent, (((0,), (1,)), ((), ())), preferred_element_type=jnp.float32
    ).astype(jnp.bfloat16)
    raw_keys = jnp.concatenate(
        [lifted[:NOPE].astype(jnp.float32), rot_key.astype(jnp.float32).T], axis=0
    )
    bundle = jnp.concatenate(
        [head_prepare(raw_keys, key_gain, cosine, sine_val), lifted[NOPE:]], axis=0
    )

    shifts = range(SIDE)
    kv_parts = [bundle] + [column_shift(bundle, k) for k in shifts[1:]]
    q_parts = [q_set] + [row_shift(q_set, k) for k in shifts[1:]]
    k_starts = jnp.stack([((my_y - k) % SIDE * SIDE + my_x) * shard_len for k in shifts])
    q_cols = [(my_x - k) % SIDE for k in shifts]
    q_starts = jnp.stack(
        sum(
            [
                [
                    (my_y * SIDE + c) * shard_len,
                    ((SIDE - 1 - my_y) * SIDE + c) * shard_len + half_len,
                ]
                for c in q_cols
            ],
            [],
        )
    )
    partial = attend(q_parts, kv_parts, q_starts.astype(jnp.int32), k_starts.astype(jnp.int32))
    pieces = [partial[0]] + [row_shift(partial[k], -k) for k in shifts[1:]]
    levels = [jnp.sum(p[VH : VH + 3].astype(jnp.float32), axis=0, keepdims=True) for p in pieces]
    top = levels[0]
    for level in levels[1:]:
        top = jnp.maximum(top, level)
    factors = [jnp.exp2(level - top) for level in levels]
    merged = sum(w * p[:VH].astype(jnp.float32) for w, p in zip(factors, pieces)) / sum(factors)
    merged = merged.astype(jnp.bfloat16)
    back = row_swap(merged[:, half_len:])
    attended = jnp.concatenate([merged[:, :half_len], back], axis=1)

    token_rows = lax.all_to_all(attended.T, "tp", split_axis=0, concat_axis=1, tiled=True)
    token_rows = token_rows.astype(jnp.float32)
    normed_rows = (token_rows * rms_scale(token_rows) * out_gain).astype(jnp.bfloat16)
    mixed = jnp.dot(normed_rows, out_weight, preferred_element_type=jnp.float32)
    middle = residual.astype(jnp.float32) + mixed
    ffn_input = (middle * rms_scale(middle) * ffn_gain).astype(jnp.bfloat16)
    slot_total = sp_count * (TILE + 1)
    targets = slot_targets(routes, sp_count)
    chooser = select_matrix(targets, slot_total)
    outbound = jnp.einsum(
        "ts,td->sd", chooser, ffn_input, preferred_element_type=jnp.float32
    ).astype(jnp.bfloat16)
    arrived = expert_exchange(to_wire(outbound, sp_count))
    my_rows = from_wire(arrived)
    their_rows = core_swap(my_rows)
    weight_pieces, places = [], []
    for h, half in enumerate(halves):
        size = half.shape[0]
        start = h * size
        for n in range(4):
            for way, ring in ((0, ahead[h]), (1, behind[h])):
                if n == 0 and way == 1:
                    continue
                weight_pieces.append(ring[n])
                places.append((2 * n - 1 + way if n else 0, start, size))
    size = halves[0].shape[0]
    weight_pieces += [ahead[0][4], behind[1][4]]
    places += [(7, 0, size), (7, size, size)]
    own_sum, other_sum = expert_ffn(my_rows, their_rows, weight_pieces, places)
    served = (
        own_sum.astype(jnp.float32) + core_swap(other_sum).astype(jnp.float32)
    ).astype(jnp.bfloat16)
    returned_rows = from_wire(expert_exchange(to_wire(served, sp_count)))
    hits = targets[:, :, None] == jnp.arange(slot_total, dtype=jnp.int32)[None, None, :]
    shares = jnp.sum(jnp.where(hits, route_weights[:, :, None], 0.0), axis=1)
    moe_sum = jnp.dot(
        shares,
        returned_rows.astype(jnp.float32),
        precision=lax.Precision.HIGHEST,
        preferred_element_type=jnp.float32,
    )
    return (middle + moe_sum).astype(jnp.bfloat16)


def solution(mesh):
    return jax.shard_map(
        shards,
        mesh=mesh,
        in_specs=(
            P("sp", "tp"),
            P("sp", None),
            P("sp", None),
            P(),
            P(None, "tp"),
            P(None, "tp"),
            P(),
            P(),
            P(),
            P(),
            P(("sp", "tp"), None),
            P(),
            P(("sp", "tp"), None),
            P(("sp", "tp"), None),
            P("sp", None, "tp"),
            P("sp", None, "tp"),
            P("sp", "tp", None),
        ),
        out_specs=P(("sp", "tp"), None),
        check_vma=False,
    )
```

```python
import jax
import jax.numpy as jnp
from jax import lax
from jax.experimental import pallas as pl
from jax.experimental.pallas import tpu as pltpu
from jax.sharding import PartitionSpec as P


D = 2048
NOPE = 64
ROPE = 32
VH = 64
QK = 96
CORES = 2
LANES = 128
TILE = 8
SIDE = 4
LOG2E = 1.4426950408889634
LOW = -1e30


epsilon = 1e-06
rope_base = 10000.0


def rms_scale(values):
    return lax.rsqrt(jnp.mean(values * values, axis=-1, keepdims=True) + epsilon)


def head_prepare(raw, gain_vec, cosine, sine_val):
    scale = lax.rsqrt(jnp.mean(raw * raw, axis=0, keepdims=True) + epsilon)
    normed = raw * scale * gain_vec[:, None]
    first = normed[NOPE : NOPE + ROPE // 2]
    second = normed[NOPE + ROPE // 2 :]
    return jnp.concatenate(
        [normed[:NOPE], first * cosine - second * sine_val, second * cosine + first * sine_val],
        axis=0,
    ).astype(jnp.bfloat16)


def attend_kernel(*refs, tq, tk, kb, parts):
    me = lax.axis_index("sp")
    my_y, my_x = me // SIDE, me % SIDE
    q_in, kv_in = refs[:parts], refs[parts : 2 * parts]
    out_refs = refs[2 * parts : 3 * parts]
    q_buf, kv_buf, k_nat, v_aug, acc, peak, out_buf, sems = refs[3 * parts :]
    span = kv_buf.shape[2]
    copies = []
    for i in range(parts):
        for j, (src, dst) in enumerate(((kv_in[i], kv_buf.at[i]), (q_in[i], q_buf.at[i]))):
            copy = pltpu.make_async_copy(src, dst, sems.at[2 * i + j])
            copy.start()
            copies.append(copy)
    for i in range(parts):
        copies[2 * i].wait()
        k_nat[pl.ds(i * span, span), :] = kv_buf[i, :QK, :].T
        for j in range(span // tk):
            piece = i * (span // tk) + j
            v_aug[piece, :VH, :] = kv_buf[i, QK:, j * tk : (j + 1) * tk]
            v_aug[piece, VH:, :] = jnp.ones((16, tk), jnp.bfloat16)
    for i in range(parts):
        copies[2 * i + 1].wait()

    scale = LOG2E * QK ** (-0.5)
    per_q = span // tq
    per_k = span // tk

    def q_tile(t, carry):
        i, h = t // per_q, t % per_q
        row = jnp.where(h == 0, my_y, SIDE - 1 - my_y)
        q_start = (row * SIDE + (my_x + SIDE - i) % SIDE) * span + h * tq
        q = q_buf[i, :, pl.ds(pl.multiple_of(h * tq, tq), tq)]
        acc[...] = jnp.zeros_like(acc)
        peak[...] = jnp.full_like(peak, LOW)

        def k_tile(u, c):
            k_row = (my_y + SIDE - u // per_k) % SIDE
            k_start = (k_row * SIDE + my_x) * span + (u % per_k) * tk

            def score(r, masked):
                keys = k_nat[pl.ds(pl.multiple_of(u * tk + r * kb, kb), kb), :]
                s = jnp.dot(keys, q, preferred_element_type=jnp.float32)
                if masked:
                    kpos = k_start + r * kb + lax.broadcasted_iota(jnp.int32, s.shape, 0)
                    qpos = q_start + lax.broadcasted_iota(jnp.int32, s.shape, 1)
                    s = jnp.where(kpos <= qpos, s, LOW)
                return s

            def update(masked):
                old, total = peak[0:1, :], acc[...]
                ahead = score(0, masked)
                for r in range(tk // kb):
                    s = ahead
                    if (r + 1) * kb < tk:
                        ahead = score(r + 1, masked)
                    new = jnp.maximum(old, jnp.max(s, axis=0, keepdims=True))
                    e = jnp.exp2((s - new) * scale).astype(jnp.bfloat16)
                    part = jnp.dot(
                        v_aug[u, :, r * kb : (r + 1) * kb], e, preferred_element_type=jnp.float32
                    )
                    total = total * jnp.exp2((old - new) * scale) + part
                    old = new
                acc[...] = total
                peak[...] = jnp.broadcast_to(old, peak.shape)

            @pl.when(k_start + tk - 1 <= q_start)
            def _():
                update(False)

            @pl.when((k_start + tk - 1 > q_start) & (k_start <= q_start + tq - 1))
            def _():
                update(True)

            return c

        lax.fori_loop(0, parts * per_k, k_tile, 0)
        total = acc[VH : VH + 1, :]
        live = total > 0.0
        safe = jnp.where(live, total, 1.0)
        lse = jnp.where(live, peak[0:1, :] * scale + jnp.log2(safe), LOW)
        hi = lse.astype(jnp.bfloat16)
        mid = (lse - hi.astype(jnp.float32)).astype(jnp.bfloat16)
        lo = (lse - hi.astype(jnp.float32) - mid.astype(jnp.float32)).astype(jnp.bfloat16)
        row = lax.broadcasted_iota(jnp.int32, (16, tq), 0)
        stats = jnp.where(
            row == 0,
            hi.astype(jnp.float32),
            jnp.where(row == 1, mid.astype(jnp.float32), jnp.where(row == 2, lo.astype(jnp.float32), 0.0)),
        )
        cols = pl.ds(pl.multiple_of(h * tq, tq), tq)
        out_buf[i, :VH, cols] = (acc[:VH, :] / safe).astype(jnp.bfloat16)
        out_buf[i, VH:, cols] = stats.astype(jnp.bfloat16)
        return carry

    lax.fori_loop(0, parts * per_q, q_tile, 0)
    for i in range(parts):
        out_refs[i][...] = out_buf[i]


def attend(q_parts, kv_parts, tq=512, tk=1024, kb=512):
    parts = len(q_parts)
    span = q_parts[0].shape[1]
    hbm = pl.BlockSpec(memory_space=pltpu.HBM)

    def kernel(*refs):
        attend_kernel(*refs, tq=tq, tk=tk, kb=kb, parts=parts)

    work = parts * parts * span * span // 2
    return pl.pallas_call(
        kernel,
        out_shape=[jax.ShapeDtypeStruct((VH + 16, span), jnp.bfloat16)] * parts,
        in_specs=[hbm] * (2 * parts),
        out_specs=[pl.BlockSpec(memory_space=pltpu.VMEM)] * parts,
        scratch_shapes=[
            pltpu.VMEM((parts, QK, span), jnp.bfloat16),
            pltpu.VMEM((parts, QK + VH, span), jnp.bfloat16),
            pltpu.VMEM((parts * span, QK), jnp.bfloat16),
            pltpu.VMEM((parts * span // tk, VH + 16, tk), jnp.bfloat16),
            pltpu.VMEM((VH + 16, tq), jnp.float32),
            pltpu.VMEM((8, tq), jnp.float32),
            pltpu.VMEM((parts, VH + 16, span), jnp.bfloat16),
            pltpu.SemaphoreType.DMA((2 * parts,)),
        ],
        compiler_params=pltpu.CompilerParams(vmem_limit_bytes=60 * 1024 * 1024),
        cost_estimate=pl.CostEstimate(
            flops=2 * work * (QK + VH), bytes_accessed=3 * 1024 * 1024, transcendentals=work
        ),
        name="attend",
    )(*q_parts, *kv_parts)


def expert_group(rows, w_buf, slots):
    width = w_buf.shape[2]
    weights = jnp.concatenate(
        [w_buf[s, :D, :] for s in slots] + [w_buf[s, D : 2 * D, :] for s in slots], axis=1
    )
    both = jnp.dot(rows, weights, preferred_element_type=jnp.float32)
    half = both.shape[1] // 2
    gate, up = both[:, :half], both[:, half:]
    hidden = (gate / (1.0 + jnp.exp(-gate)) * up).astype(jnp.bfloat16)
    down = jnp.concatenate(
        [
            jnp.concatenate(
                [w_buf[s, 2 * D + j * width : 2 * D + (j + 1) * width, :] for s in slots], axis=0
            )
            for j in range(D // LANES)
        ],
        axis=1,
    )
    return jnp.dot(hidden, down, preferred_element_type=jnp.float32)


def expert_kernel(x_ref, y_ref, *refs, places, pairs):
    total = len(places)
    w_refs, (o_ref, p_ref, acc, w_buf, sems) = refs[:total], refs[total:]
    copies = [
        pltpu.make_async_copy(w_refs[i], w_buf.at[s, pl.ds(first, size)], sems.at[i])
        for i, (s, first, size) in enumerate(places)
    ]
    for copy in copies:
        copy.start()
    rows = jnp.concatenate([x_ref[...], y_ref[...]], axis=0)
    slices = w_buf.shape[0]
    for first in range(0, slices, pairs):
        slots = list(range(first, first + pairs))
        for copy, place in zip(copies, places):
            if place[0] in slots:
                copy.wait()
        part = expert_group(rows, w_buf, slots)
        acc[...] = part if first == 0 else acc[...] + part
    count = x_ref.shape[0]
    o_ref[...] = acc[:count, :].astype(jnp.bfloat16)
    p_ref[...] = acc[count:, :].astype(jnp.bfloat16)


def expert_ffn(rows, others, pieces, places):
    count = rows.shape[0]
    slices, depth, width = 1 + max(p[0] for p in places), 3 * D, LANES
    vmem = pl.BlockSpec(memory_space=pltpu.VMEM)
    hbm = pl.BlockSpec(memory_space=pl.ANY)

    def kernel(*refs):
        expert_kernel(*refs, places=places, pairs=2)

    return pl.pallas_call(
        kernel,
        out_shape=[jax.ShapeDtypeStruct((count, D), jnp.bfloat16)] * 2,
        in_specs=[vmem, vmem] + [hbm] * len(pieces),
        out_specs=[vmem, vmem],
        scratch_shapes=[
            pltpu.VMEM((2 * count, D), jnp.float32),
            pltpu.VMEM((slices, depth, width), jnp.bfloat16),
            pltpu.SemaphoreType.DMA((len(pieces),)),
        ],
        compiler_params=pltpu.CompilerParams(vmem_limit_bytes=34 * 1024 * 1024),
        cost_estimate=pl.CostEstimate(
            flops=12 * count * D * slices * width,
            bytes_accessed=6 * D * slices * width,
            transcendentals=2 * count * slices * width,
        ),
        name="expert_ffn",
    )(rows, others, *pieces)


def to_wire(rows, peers):
    tiles = D // LANES
    main = rows[: peers * TILE].reshape(peers, TILE, tiles, LANES)
    main = main.transpose(0, 2, 1, 3).reshape(peers, tiles * TILE, LANES)
    return jnp.concatenate([main, rows[peers * TILE :].reshape(peers, tiles, LANES)], axis=1)


def from_wire(wire):
    peers = wire.shape[0]
    tiles = D // LANES
    main = wire[:, : tiles * TILE].reshape(peers, tiles, TILE, LANES)
    main = main.transpose(0, 2, 1, 3).reshape(peers * TILE, D)
    return jnp.concatenate([main, wire[:, tiles * TILE :].reshape(peers, D)], axis=0)


def slot_targets(route_rows, expert_total):
    flat_routes = route_rows.reshape(-1)
    one_hot = (flat_routes[:, None] == jnp.arange(expert_total, dtype=jnp.int32)[None, :]).astype(
        jnp.int32
    )
    earlier = jnp.cumsum(one_hot, axis=0) - one_hot
    rank_in = jnp.sum(earlier * one_hot, axis=1)
    slots = jnp.where(
        rank_in < TILE, flat_routes * TILE + rank_in, expert_total * TILE + flat_routes
    )
    return slots.reshape(route_rows.shape)


def select_matrix(targets, slot_total):
    hits = targets[:, :, None] == jnp.arange(slot_total, dtype=jnp.int32)[None, None, :]
    return jnp.sum(hits.astype(jnp.bfloat16), axis=1)


def row_shift(value, k):
    pairs = [
        (y * SIDE + x, y * SIDE + (x + k) % SIDE) for y in range(SIDE) for x in range(SIDE)
    ]
    return lax.ppermute(value, "sp", pairs)


def column_shift(value, k):
    pairs = [
        (y * SIDE + x, ((y + k) % SIDE) * SIDE + x) for y in range(SIDE) for x in range(SIDE)
    ]
    return lax.ppermute(value, "sp", pairs)


def row_swap(value):
    pairs = [
        (y * SIDE + x, (SIDE - 1 - y) * SIDE + x) for y in range(SIDE) for x in range(SIDE)
    ]
    return lax.ppermute(value, "sp", pairs)


def expert_exchange(wire):
    return lax.all_to_all(wire, "sp", split_axis=0, concat_axis=0, tiled=True)


def z_shift(value, k):
    count = lax.axis_size("tp")
    return lax.ppermute(value, "tp", [(t, (t + CORES * k) % count) for t in range(count)])


def core_swap(value):
    pairs = [(t, t ^ 1) for t in range(lax.axis_size("tp"))]
    return lax.ppermute(value, "tp", pairs)


def shards(
    queries,
    latent,
    rot_key,
    latent_gain,
    key_up,
    value_up,
    query_gain,
    key_gain,
    out_gain,
    out_weight,
    residual,
    ffn_gain,
    routes,
    route_weights,
    expert_gate,
    expert_up,
    expert_down,
):
    shard_len = queries.shape[0]
    half_len = shard_len // 2
    sp_count = lax.axis_size("sp")
    me = lax.axis_index("sp")

    gate, up, down = expert_gate[0], expert_up[0], expert_down[0]
    down = down.reshape(down.shape[0], D // LANES, LANES).transpose(1, 0, 2).reshape(-1, LANES)
    halves = [
        jnp.concatenate([gate, up[: D // 2]], axis=0),
        jnp.concatenate([up[D // 2 :], down], axis=0),
    ]
    ahead, behind = [[half] for half in halves], [[half] for half in halves]

    def ring_step(h, n):
        front, back = ahead[h][-1], behind[h][-1]
        if n < 4 or h == 0:
            ahead[h].append(z_shift(front, 1))
        if n < 4 or h == 1:
            behind[h].append(z_shift(back, -1))

    for n in (1, 2, 3, 4):
        for h in (0, 1):
            ring_step(h, n)

    positions = me * shard_len + jnp.arange(shard_len, dtype=jnp.int32)
    inverse = rope_base ** (-jnp.arange(0, ROPE, 2, dtype=jnp.float32) / ROPE)
    angles = positions.astype(jnp.float32)[None, :] * inverse[:, None]
    cosine, sine_val = jnp.cos(angles), jnp.sin(angles)

    query_rows = head_prepare(queries.astype(jnp.float32).T, query_gain, cosine, sine_val)
    swapped = row_swap(query_rows[:, half_len:])
    q_set = jnp.concatenate([query_rows[:, :half_len], swapped], axis=1)

    lat_f32 = latent.astype(jnp.float32)
    normed_latent = (lat_f32 * rms_scale(lat_f32) * latent_gain).astype(jnp.bfloat16)
    both_up = jnp.concatenate([key_up, value_up], axis=1)
    lifted = lax.dot_general(
        both_up, normed_latent, (((0,), (1,)), ((), ())), preferred_element_type=jnp.float32
    ).astype(jnp.bfloat16)
    raw_keys = jnp.concatenate(
        [lifted[:NOPE].astype(jnp.float32), rot_key.astype(jnp.float32).T], axis=0
    )
    bundle = jnp.concatenate(
        [head_prepare(raw_keys, key_gain, cosine, sine_val), lifted[NOPE:]], axis=0
    )

    shifts = range(SIDE)
    kv_parts = [bundle] + [column_shift(bundle, k) for k in shifts[1:]]
    q_parts = [q_set] + [row_shift(q_set, k) for k in shifts[1:]]
    partial = attend(q_parts, kv_parts)
    pieces = [partial[0]] + [row_shift(partial[k], -k) for k in shifts[1:]]
    levels = [
        sum(p[VH + j : VH + j + 1].astype(jnp.float32) for j in range(3)) for p in pieces
    ]
    top = levels[0]
    for level in levels[1:]:
        top = jnp.maximum(top, level)
    factors = [jnp.exp2(level - top) for level in levels]
    merged = sum(w * p[:VH].astype(jnp.float32) for w, p in zip(factors, pieces)) / sum(factors)
    merged = merged.astype(jnp.bfloat16)
    back = row_swap(merged[:, half_len:])
    attended = jnp.concatenate([merged[:, :half_len], back], axis=1)

    token_rows = lax.all_to_all(attended.T, "tp", split_axis=0, concat_axis=1, tiled=True)
    token_rows = token_rows.astype(jnp.float32)
    normed_rows = (token_rows * rms_scale(token_rows) * out_gain).astype(jnp.bfloat16)
    mixed = jnp.dot(normed_rows, out_weight, preferred_element_type=jnp.float32)
    middle = residual.astype(jnp.float32) + mixed
    ffn_input = (middle * rms_scale(middle) * ffn_gain).astype(jnp.bfloat16)
    slot_total = sp_count * (TILE + 1)
    targets = slot_targets(routes, sp_count)
    chooser = select_matrix(targets, slot_total)
    outbound = jnp.einsum(
        "ts,td->sd", chooser, ffn_input, preferred_element_type=jnp.float32
    ).astype(jnp.bfloat16)
    arrived = expert_exchange(to_wire(outbound, sp_count))
    my_rows = from_wire(arrived)
    their_rows = core_swap(my_rows)
    weight_pieces, places = [], []
    for h, half in enumerate(halves):
        size = half.shape[0]
        start = h * size
        for n in range(4):
            for way, ring in ((0, ahead[h]), (1, behind[h])):
                if n == 0 and way == 1:
                    continue
                weight_pieces.append(ring[n])
                places.append((2 * n - 1 + way if n else 0, start, size))
    size = halves[0].shape[0]
    weight_pieces += [ahead[0][4], behind[1][4]]
    places += [(7, 0, size), (7, size, size)]
    own_sum, other_sum = expert_ffn(my_rows, their_rows, weight_pieces, places)
    served = (
        own_sum.astype(jnp.float32) + core_swap(other_sum).astype(jnp.float32)
    ).astype(jnp.bfloat16)
    returned_rows = from_wire(expert_exchange(to_wire(served, sp_count)))
    hits = targets[:, :, None] == jnp.arange(slot_total, dtype=jnp.int32)[None, None, :]
    shares = jnp.sum(jnp.where(hits, route_weights[:, :, None], 0.0), axis=1)
    moe_sum = jnp.dot(
        shares,
        returned_rows.astype(jnp.float32),
        precision=lax.Precision.HIGHEST,
        preferred_element_type=jnp.float32,
    )
    return (middle + moe_sum).astype(jnp.bfloat16)


def solution(mesh):
    return jax.shard_map(
        shards,
        mesh=mesh,
        in_specs=(
            P("sp", "tp"),
            P("sp", None),
            P("sp", None),
            P(),
            P(None, "tp"),
            P(None, "tp"),
            P(),
            P(),
            P(),
            P(),
            P(("sp", "tp"), None),
            P(),
            P(("sp", "tp"), None),
            P(("sp", "tp"), None),
            P("sp", None, "tp"),
            P("sp", None, "tp"),
            P("sp", "tp", None),
        ),
        out_specs=P(("sp", "tp"), None),
        check_vma=False,
    )
```
